512 devices in a mesh: grp: 2 (over y), fs: 32 (over z, core), tp: 8 (over x).
Axes of the slice: x: 8, y: 2, z: 16, core: 2. Of those that a mesh axis runs over, the one named last changes fastest.
The devices are a block of a 8x8x16 slice.
Arguments:
- tokens: bfloat16 [24576, 2048], P(('grp', 'fs'), 'tp'), parts along dimension 0, may hold values from -6 to 6
- norm_gain: float32 [2048], P('fs'), may hold values from 0.1 to 1.9
- gate_weight: float32 [32, 2048, 1024], P(None, 'fs', 'tp'), may hold values from -0.125 to 0.125
- up_weight: float32 [32, 2048, 1024], P(None, 'fs', 'tp'), may hold values from -0.125 to 0.125
- down_weight: float32 [32, 1024, 2048], P(None, 'fs', 'tp'), may hold values from -0.1875 to 0.1875
- routes: int32 [24576, 2], P(('grp', 'fs')), parts along dimension 0, may hold values from 0 to 31, as said below
- route_weights: float32 [24576, 2], P(('grp', 'fs')), parts along dimension 0, may hold values from 0.2 to 1
Outputs:
- gate_serve: bfloat16 [64, 2048, 1024], P(('grp', 'fs'), None, 'tp'), parts along dimension 0
- up_serve: bfloat16 [64, 2048, 1024], P(('grp', 'fs'), None, 'tp'), parts along dimension 0
- down_serve: bfloat16 [64, 1024, 2048], P(('grp', 'fs'), None, 'tp'), parts along dimension 0
- mixture: bfloat16 [24576, 2048], P(('grp', 'fs'), 'tp'), parts along dimension 0
The draws below stay inside these ranges and needn't reach their ends.
There are 2 independent parts, one for each index of `grp`. The reference program is written for one: setup_inputs(seed, part) draws one part's arguments, and reference() takes and returns one part's arrays. A program takes and returns all parts, laid end to end along the dimension named above; an argument that names none is the same for every part. Nothing has to cross between parts.
Inputs may be any that keep to these rules, and one draw needn't show every extreme that they name: `routes`: each row names two different experts of one group (expert e lies in group e // 8). In each aligned block of 384 rows no expert is named more than 36 times, and every expert of one group is named exactly 36 times.
All inputs are finite; a program needn't handle non-finite values.
Results may differ from the reference program's by a relative error of at most 0.0087.
Values may be sent and summed in bfloat16 or wider, within the bound.
No kernel may reach another device: no remote copies, remote signals or barrier semaphores. Data moves between devices by JAX's collectives and lax.ppermute only.
A program may use at most 64 MiB of HBM per device.

```python
import jax
import jax.numpy as jnp
from jax import lax

D = 2048
DE = 1024
NGROUPS = 4
EPG = 8
TOK_DEV = 384
EXPERTS = 32
CAP = 36
TOKENS = 12288


def block_routes(block_key):
    subkeys = jax.random.split(block_key, 6)
    eighth = TOK_DEV // 8
    first_count = jax.random.randint(subkeys[0], (), eighth, 2 * eighth + 1, dtype=jnp.int32)
    second_count = jax.random.randint(subkeys[1], (), eighth, 2 * eighth + 1, dtype=jnp.int32)
    counts = jnp.stack([jnp.int32(3 * eighth), first_count, second_count, jnp.int32(5 * eighth) - first_count - second_count]).astype(jnp.int32)
    starts = (jnp.cumsum(counts) - counts).astype(jnp.int32)
    places = jnp.arange(TOK_DEV, dtype=jnp.int32)
    order_slot = jnp.sum((places[:, None] >= starts[None, 1:]).astype(jnp.int32), axis=1).astype(jnp.int32)
    rank_in_group = places - starts[order_slot]
    group_order = jax.random.permutation(subkeys[2], NGROUPS).astype(jnp.int32)
    group_id = group_order[order_slot]
    member_keys = jax.random.split(subkeys[3], NGROUPS)
    member_perm = jax.vmap(lambda member_key: jax.random.permutation(member_key, EPG))(member_keys).astype(jnp.int32)
    shifts = jax.random.randint(subkeys[4], (NGROUPS, TOK_DEV // EPG + 1), 0, EPG - 1, dtype=jnp.int32)
    lead_member = rank_in_group % EPG
    partner = (rank_in_group + 1 + shifts[order_slot, rank_in_group // EPG]) % EPG
    first_expert = group_id * EPG + member_perm[group_id, lead_member]
    second_expert = group_id * EPG + member_perm[group_id, partner]
    expert_pairs = jnp.stack([first_expert, second_expert], axis=1).astype(jnp.int32)
    shuffle = jax.random.permutation(subkeys[5], TOK_DEV).astype(jnp.int32)
    return jnp.zeros((TOK_DEV, 2), jnp.int32).at[shuffle].set(expert_pairs)


def draw_routes(key, part):
    block_keys = jax.random.split(jax.random.fold_in(key, 17), TOKENS // TOK_DEV)
    return jax.vmap(block_routes)(block_keys).reshape(TOKENS, 2).astype(jnp.int32)


def level_of(rng, shape, shards, smallest, high):
    factor_of = 1.0
    for dim, parts in shards:
        steps = jax.random.uniform(jax.random.fold_in(jax.random.fold_in(rng, 6), dim), (parts,), jnp.float32, smallest / len(shards), high / len(shards))
        factor_of = factor_of * jnp.repeat(jnp.exp(steps), shape[dim] // parts).reshape((-1,) + (1,) * (len(shape) - 1 - dim))
    return factor_of


def normal_values(rng, dims, scale, bound, shards=(), held_as=jnp.bfloat16):
    array = scale * jax.random.normal(rng, dims, jnp.float32)
    if shards:
        array = array * level_of(rng, dims, shards, -0.22, 0.18)
    return jnp.clip(array, -bound, bound).astype(held_as)


def setup_inputs(seed: int = 0, part: int = 0) -> dict:
    splits = jax.random.split(jax.random.key(seed), 8)
    part_keys = jax.random.split(jax.random.fold_in(splits[7], part), 8)
    return {
        "tokens": normal_values(part_keys[0], (TOKENS, D), 1.0, 6.0, ((0, 32), (1, 8))),
        "norm_gain": jnp.clip(1.0 + 0.18 * jax.random.normal(splits[1], (D,), jnp.float32), 0.1, 1.9),
        "gate_weight": normal_values(splits[2], (EXPERTS, D, DE), D ** -0.5, 0.125, ((1, 32), (2, 8)), jnp.float32),
        "up_weight": normal_values(splits[3], (EXPERTS, D, DE), D ** -0.5, 0.125, ((1, 32), (2, 8)), jnp.float32),
        "down_weight": normal_values(splits[4], (EXPERTS, DE, D), DE ** -0.5, 0.1875, ((1, 32), (2, 8)), jnp.float32),
        "routes": draw_routes(jax.random.fold_in(jax.random.fold_in(splits[7], part), 71), part),
        "route_weights": jnp.clip(0.2 + 0.8 * jax.random.uniform(part_keys[6], (TOKENS, 2), jnp.float32) ** level_of(part_keys[6], (TOKENS, 2), ((0, 32),), -0.2, 0.2), 0.2, 1.0),
    }


epsilon = 1e-06

def normalize(rows):
    values = rows.astype(jnp.float32)
    scale = lax.rsqrt(lax.optimization_barrier(jnp.mean(values * values, axis=-1, keepdims=True)) + epsilon)
    return (values * scale).astype(jnp.bfloat16)

def reference(tokens, norm_gain, gate_weight, up_weight, down_weight, routes, route_weights):
    gate_serve = (norm_gain[None, :, None] * gate_weight).astype(jnp.bfloat16)
    up_serve = (norm_gain[None, :, None] * up_weight).astype(jnp.bfloat16)
    down_serve = down_weight.astype(jnp.bfloat16)
    normed = normalize(tokens)
    blocks = TOKENS // TOK_DEV
    span = blocks * CAP
    flat_routes = routes.reshape(blocks, TOK_DEV * 2)
    expert_ids = jnp.arange(EXPERTS, dtype=jnp.int32)
    onehot = (flat_routes[:, :, None] == expert_ids[None, None, :]).astype(jnp.int32)
    position = lax.optimization_barrier(jnp.sum((jnp.cumsum(onehot, axis=1) - 1) * onehot, axis=2)).astype(jnp.int32)
    block_ids = jnp.arange(blocks, dtype=jnp.int32)[:, None]
    destination = (flat_routes * span + block_ids * CAP + position).astype(jnp.int32)
    token_ids = block_ids * TOK_DEV + (jnp.arange(TOK_DEV * 2, dtype=jnp.int32) // 2)[None, :]
    table = jnp.full((EXPERTS * span,), TOKENS, jnp.int32)
    table = table.at[destination.reshape(-1)].set(token_ids.reshape(-1).astype(jnp.int32))
    padded = jnp.concatenate([normed, jnp.zeros((1, D), jnp.bfloat16)], axis=0)

    def expert_rows(operands):
        index_rows, gate_matrix, up_matrix, down_matrix = operands
        rows = padded[index_rows]
        gate_part = jnp.dot(rows, gate_matrix, preferred_element_type=jnp.float32)
        up_part = jnp.dot(rows, up_matrix, preferred_element_type=jnp.float32)
        hidden = (jax.nn.silu(gate_part) * up_part).astype(jnp.bfloat16)
        return jnp.dot(hidden, down_matrix, preferred_element_type=jnp.float32).astype(jnp.bfloat16)
    outputs = lax.map(expert_rows, (table.reshape(EXPERTS, span), gate_serve, up_serve, down_serve))
    picked = outputs.reshape(EXPERTS * span, D)[destination.reshape(TOKENS, 2)]
    mixture = lax.optimization_barrier(jnp.sum(route_weights[:, :, None] * picked.astype(jnp.float32), axis=1)).astype(jnp.bfloat16)
    return (gate_serve, up_serve, down_serve, mixture)
```

```python
import jax
import jax.numpy as jnp
from jax import lax
from jax.experimental import pallas as pl
from jax.experimental.pallas import tpu as pltpu
from jax.sharding import PartitionSpec as P


CAP = 36
MAIN = 32
SLAB = 72
HALF = 128
BF16 = jnp.bfloat16
F32 = jnp.float32
epsilon = 1e-06


def route_kernel(routes, tokens, outbound, rows):
    experts = outbound.shape[0] // SLAB
    n_tok = tokens.shape[0]
    first, second = routes[0:1, :], routes[1:2, :]
    ids = lax.broadcasted_iota(jnp.int32, (experts, n_tok), 0)
    hit0 = (ids == first).astype(F32)
    hit1 = (ids == second).astype(F32)
    before = (
        lax.broadcasted_iota(jnp.int32, (n_tok, n_tok), 0)
        < lax.broadcasted_iota(jnp.int32, (n_tok, n_tok), 1)
    ).astype(F32).astype(BF16)
    count0 = jnp.dot(hit0.astype(BF16), before, preferred_element_type=F32)
    count1 = jnp.dot(hit1.astype(BF16), before, preferred_element_type=F32)
    count1 = count1 + jnp.sum(hit0, axis=1, keepdims=True)
    slot0 = jnp.sum(hit0 * count0, axis=0, keepdims=True).astype(jnp.int32)
    slot1 = jnp.sum(hit1 * count1, axis=0, keepdims=True).astype(jnp.int32)
    low0 = first * SLAB + jnp.where(slot0 < MAIN, slot0, slot0 + MAIN)
    low1 = second * SLAB + jnp.where(slot1 < MAIN, slot1, slot1 + MAIN)
    high0 = low0 + jnp.where(slot0 < MAIN, MAIN, CAP - MAIN)
    high1 = low1 + jnp.where(slot1 < MAIN, MAIN, CAP - MAIN)
    rows[...] = jnp.concatenate([low0, low1, high0, high1, low0, low1, high0, high1], axis=0)
    part = 8 * SLAB
    left, right = tokens[:, :HALF], tokens[:, HALF:]
    for g in range(experts // 8):
        ids = lax.broadcasted_iota(jnp.int32, (part, n_tok), 0) + g * part
        low = jnp.logical_or(ids == low0, ids == low1).astype(F32).astype(BF16)
        high = jnp.logical_or(ids == high0, ids == high1).astype(F32).astype(BF16)
        out = jnp.dot(low, left, preferred_element_type=F32)
        out = out + jnp.dot(high, right, preferred_element_type=F32)
        outbound[g * part : (g + 1) * part, :] = out.astype(BF16)


def tile_row(shape):
    return lax.broadcasted_iota(jnp.int32, shape, len(shape) - 2)


def ffn_kernel(me, *refs):
    half_a, half_b, weights = refs[0:9], refs[9:18], refs[18]
    hidden, gate_out, up_out = refs[19:22]
    i = pl.program_id(0)
    n_tp = 8
    offsets = (0, -1, 1, -2, 2, -3, 3, 4)
    pairs = 8 * MAIN
    acc = jnp.zeros((pairs, 2 * HALF), F32)
    rest0 = jnp.zeros((64, 2 * HALF), F32)
    rest1 = jnp.zeros((64, 2 * HALF), F32)
    square = jnp.zeros((pairs, HALF), F32)
    square_rest = jnp.zeros((64, HALF), F32)
    for n, offset in enumerate(offsets):
        if n < 7:
            x = jnp.where(i < 2, half_a[n][...], half_b[n][...])
        else:
            x = jnp.where(
                i < 2,
                jnp.where(i == 0, half_a[7][...], half_a[8][...]),
                jnp.where(i == 2, half_b[7][...], half_b[8][...]),
            )
        x = x.reshape(8, SLAB, HALF)
        left = x[:, :MAIN].reshape(pairs, HALF)
        right = x[:, MAIN : 2 * MAIN].reshape(pairs, HALF)
        rest = x[:, 2 * MAIN :].reshape(64, HALF)
        source = (me[0] + offset + n_tp) % n_tp
        w = weights[pl.ds(pl.multiple_of(source * 256, 256), 256), :]
        both = jnp.concatenate([left, right], axis=1)
        acc = acc + jnp.dot(both, w, preferred_element_type=F32)
        rest0 = rest0 + jnp.dot(rest, w[:HALF], preferred_element_type=F32)
        rest1 = rest1 + jnp.dot(rest, w[HALF:], preferred_element_type=F32)
        l32, r32, s32 = left.astype(F32), right.astype(F32), rest.astype(F32)
        square = square + (l32 * l32 + r32 * r32)
        square_rest = square_rest + s32 * s32
    features = weights.shape[0]

    def activate(part, total):
        scale = lax.rsqrt(total * (1.0 / features) + epsilon)
        gate = part[:, :HALF] * scale
        up = part[:, HALF:] * scale
        return gate / (1.0 + jnp.exp(-gate)) * up

    main = activate(acc, jnp.sum(square, axis=1, keepdims=True))
    low = tile_row((8, 8, 2 * HALF)) < CAP - MAIN
    part = jnp.where(low, rest0.reshape(8, 8, 2 * HALF), rest1.reshape(8, 8, 2 * HALF))
    part = (part + pltpu.roll(part, 4, 1)).reshape(64, 2 * HALF)
    total = jnp.broadcast_to(jnp.sum(square_rest, axis=1, keepdims=True), (64, HALF)).reshape(8, 8, HALF)
    total = (total + pltpu.roll(total, 4, 1)).reshape(64, HALF)
    extra = activate(part, total).reshape(4, 2, 8, HALF)
    extra = jnp.where(tile_row((4, 8, HALF)) < CAP - MAIN, extra[:, 0], extra[:, 1]).reshape(32, HALF)
    hidden[0:pairs, :] = main.astype(BF16)
    hidden[pairs:, :] = extra.astype(BF16)
    share = gate_out.shape[0]
    w = weights[pl.ds(pl.multiple_of(i * share, share), share), :]
    gate_out[...] = w[:, :HALF]
    up_out[...] = w[:, HALF:]


def down_kernel(me, *refs):
    chunks, weights, out, down_out = refs[0:9], refs[9], refs[10], refs[11]
    i = pl.program_id(0)
    n_tp = 8
    offsets = (0, -1, 1, -2, 2, -3, 3, 4)
    pairs = 8 * MAIN
    acc = jnp.zeros((pairs + 32, 2 * HALF), F32)
    for n, offset in enumerate(offsets):
        h = chunks[n][...] if n < 7 else jnp.where(i < 2, chunks[7][...], chunks[8][...])
        source = (me[0] + offset + n_tp) % n_tp
        w = weights[pl.ds(pl.multiple_of(source * HALF, HALF), HALF), :]
        acc = acc + jnp.dot(h, w, preferred_element_type=F32)
    left = acc[:pairs, :HALF].reshape(8, MAIN, HALF)
    right = acc[:pairs, HALF:].reshape(8, MAIN, HALF)
    rest_l = acc[pairs:, :HALF].reshape(4, 8, HALF)
    rest_r = acc[pairs:, HALF:].reshape(4, 8, HALF)
    low = tile_row((4, 8, HALF)) < CAP - MAIN
    even = jnp.where(low, rest_l, pltpu.roll(rest_r, 4, 1))
    odd = jnp.where(low, pltpu.roll(rest_l, 4, 1), rest_r)
    rest = jnp.stack([even, odd], axis=1).reshape(8, 8, HALF)
    out[:, 0:MAIN, :] = left.astype(BF16)
    out[:, MAIN : 2 * MAIN, :] = right.astype(BF16)
    out[:, 2 * MAIN :, :] = rest.astype(BF16)
    share = down_out.shape[0]
    down_out[...] = weights[pl.ds(pl.multiple_of(i * share, share), share), :]


def combine_kernel(rows, gains, returned, mixture):
    n_tok = rows.shape[0]
    slots = returned.shape[0]
    ids = lax.broadcasted_iota(jnp.int32, (n_tok, slots), 1)

    def pick(n):
        onehot = (ids == rows[:, n : n + 1]).astype(F32).astype(BF16)
        return jnp.dot(onehot, returned[...], preferred_element_type=F32)

    gain0, gain1 = gains[:, 0:1], gains[:, 1:2]
    mixture[:, :HALF] = (gain0 * pick(0) + gain1 * pick(1)).astype(BF16)
    mixture[:, HALF:] = (gain0 * pick(2) + gain1 * pick(3)).astype(BF16)


def all_to_all(x):
    return lax.all_to_all(x, "fs", split_axis=0, concat_axis=0, tiled=True)


def ring(x):
    n = lax.axis_size("tp")

    def step(v, side):
        shift = 1 if side == "r" else -1
        return lax.ppermute(v, "tp", [(d, (d + shift) % n) for d in range(n)])

    half = x.shape[0] // 2
    r1, l1 = step(x, "r"), step(x, "l")
    r2, l2 = step(r1, "r"), step(l1, "l")
    r3, l3 = step(r2, "r"), step(l2, "l")
    r4, l4 = step(r3[:half], "r"), step(l3[half:], "l")
    return (x, r1, l1, r2, l2, r3, l3, r4, l4)


def mixture_of_experts(tokens, norm_gain, gate_weight, up_weight, down_weight, routes, route_weights):
    experts, _, cols = gate_weight.shape
    n_tok = tokens.shape[0]
    features = tokens.shape[1] * lax.axis_size("tp")
    me = lax.axis_index("tp").reshape(1).astype(jnp.int32)
    smem = pl.BlockSpec(memory_space=pltpu.SMEM)
    outbound, rows = pl.pallas_call(
        route_kernel,
        out_shape=(
            jax.ShapeDtypeStruct((experts * SLAB, HALF), BF16),
            jax.ShapeDtypeStruct((8, n_tok), jnp.int32),
        ),
        name="route",
    )(routes.T, tokens)
    arrived = all_to_all(outbound.reshape(experts, SLAB, HALF)).reshape(experts * SLAB, HALF)
    gain = norm_gain[None, :, None]
    both_low = jnp.concatenate([gain * gate_weight, gain * up_weight], axis=2).astype(BF16)
    both_serve = all_to_all(both_low).reshape(features, 2 * cols)
    cut = experts * SLAB // 2
    halves = ring(arrived[:cut]) + ring(arrived[cut:])
    quarter = cut // 2

    def spec_a(n):
        if n < 7:
            return pl.BlockSpec((quarter, HALF), lambda i: (jnp.minimum(i, 1), 0))
        return pl.BlockSpec((quarter, HALF), lambda i: (0, 0))

    def spec_b(n):
        if n < 7:
            return pl.BlockSpec((quarter, HALF), lambda i: (jnp.maximum(i - 2, 0), 0))
        return pl.BlockSpec((quarter, HALF), lambda i: (0, 0))

    row_share = experts * CAP // 4
    hidden, gate_serve, up_serve = pl.pallas_call(
        ffn_kernel,
        grid=(4,),
        in_specs=[smem]
        + [spec_a(n) for n in range(9)]
        + [spec_b(n) for n in range(9)]
        + [pl.BlockSpec((features, 2 * cols), lambda i: (0, 0))],
        out_specs=(
            pl.BlockSpec((row_share, cols), lambda i: (i, 0)),
            pl.BlockSpec((features // 4, cols), lambda i: (i, 0)),
            pl.BlockSpec((features // 4, cols), lambda i: (i, 0)),
        ),
        out_shape=(
            jax.ShapeDtypeStruct((experts * CAP, cols), BF16),
            jax.ShapeDtypeStruct((features, cols), BF16),
            jax.ShapeDtypeStruct((features, cols), BF16),
        ),
        name="ffn",
    )(me, *halves, both_serve)
    down_low = down_weight.astype(BF16)
    down_cols = down_low.shape[2]
    down_both = all_to_all(down_low).reshape(-1, down_cols)
    inner = down_both.shape[0]
    chunks = ring(hidden)

    def spec_h(n):
        if n < 7:
            return pl.BlockSpec((row_share, cols), lambda i: (i, 0))
        if n == 7:
            return pl.BlockSpec((row_share, cols), lambda i: (jnp.minimum(i, 1), 0))
        return pl.BlockSpec((row_share, cols), lambda i: (jnp.maximum(i - 2, 0), 0))

    expert_out, down_serve = pl.pallas_call(
        down_kernel,
        grid=(4,),
        in_specs=[smem]
        + [spec_h(n) for n in range(9)]
        + [pl.BlockSpec((inner, down_cols), lambda i: (0, 0))],
        out_specs=(
            pl.BlockSpec((experts // 4, SLAB, HALF), lambda i: (i, 0, 0)),
            pl.BlockSpec((inner // 4, down_cols), lambda i: (i, 0)),
        ),
        out_shape=(
            jax.ShapeDtypeStruct((experts, SLAB, HALF), BF16),
            jax.ShapeDtypeStruct((inner, down_cols), BF16),
        ),
        name="down",
    )(me, *chunks, down_both)
    returned = all_to_all(expert_out).reshape(experts * SLAB, HALF)
    mixture = pl.pallas_call(
        combine_kernel,
        out_shape=jax.ShapeDtypeStruct(tokens.shape, BF16),
        name="combine",
    )(rows.T, route_weights, returned)
    return (gate_serve[None], up_serve[None], down_serve[None], mixture)


def solution(mesh):
    block = ("grp", "fs")
    return jax.shard_map(
        mixture_of_experts,
        mesh=mesh,
        in_specs=(
            P(block, "tp"),
            P("fs"),
            P(None, "fs", "tp"),
            P(None, "fs", "tp"),
            P(None, "fs", "tp"),
            P(block, None),
            P(block, None),
        ),
        out_specs=(
            P(block, None, "tp"),
            P(block, None, "tp"),
            P(block, None, "tp"),
            P(block, "tp"),
        ),
        check_vma=False,
    )
```

```python
import jax
import jax.numpy as jnp
from jax import lax
from jax.experimental import pallas as pl
from jax.experimental.pallas import tpu as pltpu
from jax.sharding import PartitionSpec as P


CAP = 36
MAIN = 32
SLAB = 72
HALF = 128
BF16 = jnp.bfloat16
F32 = jnp.float32
epsilon = 1e-06


def tile_row(shape):
    return lax.broadcasted_iota(jnp.int32, shape, len(shape) - 2)


def from_slabs(x):
    x = x.reshape(8, SLAB, HALF)
    left = x[:, :MAIN].reshape(8 * MAIN, HALF)
    right = x[:, MAIN : 2 * MAIN].reshape(8 * MAIN, HALF)
    rest = x[:, 2 * MAIN :].astype(F32).reshape(4, 2, 8, HALF)
    even, odd = rest[:, 0], rest[:, 1]
    low = tile_row((4, 8, HALF)) < CAP - MAIN
    rest_l = jnp.where(low, even, pltpu.roll(odd, 4, 1)).reshape(32, HALF).astype(BF16)
    rest_r = jnp.where(low, pltpu.roll(even, 4, 1), odd).reshape(32, HALF).astype(BF16)
    return jnp.concatenate([left, rest_l], axis=0), jnp.concatenate([right, rest_r], axis=0)


def to_slabs(rows, out, first):
    pairs = 8 * MAIN
    rest_l = rows[pairs:, :HALF].reshape(4, 8, HALF)
    rest_r = rows[pairs:, HALF:].reshape(4, 8, HALF)
    low = tile_row((4, 8, HALF)) < CAP - MAIN
    even = jnp.where(low, rest_l, pltpu.roll(rest_r, 4, 1))
    odd = jnp.where(low, pltpu.roll(rest_l, 4, 1), rest_r)
    rest = jnp.stack([even, odd], axis=1).reshape(8, 8, HALF)
    out[first : first + 8, 0:MAIN, :] = rows[:pairs, :HALF].reshape(8, MAIN, HALF).astype(BF16)
    out[first : first + 8, MAIN : 2 * MAIN, :] = rows[:pairs, HALF:].reshape(8, MAIN, HALF).astype(BF16)
    out[first : first + 8, 2 * MAIN :, :] = rest.astype(BF16)


def route_kernel(routes, tokens, outbound, rows):
    experts = outbound.shape[0]
    n_tok = tokens.shape[0]
    first, second = routes[0:1, :], routes[1:2, :]
    ids = lax.broadcasted_iota(jnp.int32, (experts, n_tok), 0)
    hit0 = (ids == first).astype(F32)
    hit1 = (ids == second).astype(F32)
    before = (
        lax.broadcasted_iota(jnp.int32, (n_tok, n_tok), 0)
        < lax.broadcasted_iota(jnp.int32, (n_tok, n_tok), 1)
    ).astype(F32).astype(BF16)
    count0 = jnp.dot(hit0.astype(BF16), before, preferred_element_type=F32)
    count1 = jnp.dot(hit1.astype(BF16), before, preferred_element_type=F32)
    count1 = count1 + jnp.sum(hit0, axis=1, keepdims=True)

    def row_of(expert, hit, count):
        slot = jnp.sum(hit * count, axis=0, keepdims=True).astype(jnp.int32)
        base = jnp.right_shift(expert, 3) * (8 * CAP)
        within = jnp.bitwise_and(expert, 7)
        main = within * MAIN + slot
        rest = 8 * MAIN + within * (CAP - MAIN) + (slot - MAIN)
        return base + jnp.where(slot < MAIN, main, rest)

    row0, row1 = row_of(first, hit0, count0), row_of(second, hit1, count1)
    rows[...] = jnp.concatenate([row0, row1] * 4, axis=0)
    part = 8 * CAP
    for g in range(experts // 8):
        ids = lax.broadcasted_iota(jnp.int32, (part, n_tok), 0) + g * part
        select = jnp.logical_or(ids == row0, ids == row1).astype(F32).astype(BF16)
        out = jnp.dot(select, tokens[...], preferred_element_type=F32)
        to_slabs(out, outbound, 8 * g)


def offsets_of(me):
    n_tp = 8
    return [(me + offset + n_tp) % n_tp for offset in (0, -1, 1, -2, 2, -3, 3, 4)]


def ffn_kernel(me, *refs):
    halves, weights, hidden = (refs[0:8], refs[8:16]), refs[16], refs[17]
    sources = offsets_of(me[0])
    features = weights.shape[0]
    part, slabs = 8 * CAP, 8 * SLAB
    for g in range(4):
        acc = jnp.zeros((part, 2 * HALF), F32)
        square = jnp.zeros((part, HALF), F32)
        for source, chunk in zip(sources, halves[g // 2]):
            left, right = from_slabs(chunk[(g % 2) * slabs : (g % 2 + 1) * slabs, :])
            w = weights[pl.ds(pl.multiple_of(source * 256, 256), 256), :]
            both = jnp.concatenate([left, right], axis=1)
            acc = acc + jnp.dot(both, w, preferred_element_type=F32)
            l32, r32 = left.astype(F32), right.astype(F32)
            square = square + (l32 * l32 + r32 * r32)
        total = jnp.sum(square, axis=1, keepdims=True)
        scale = lax.rsqrt(total * (1.0 / features) + epsilon)
        gate = acc[:, :HALF] * scale
        up = acc[:, HALF:] * scale
        value = gate / (1.0 + jnp.exp(-gate)) * up
        hidden[g * part : (g + 1) * part, :] = value.astype(BF16)


def down_kernel(me, *refs):
    chunks, weights, out = refs[0:8], refs[8], refs[9]
    sources = offsets_of(me[0])
    part = 8 * CAP
    pairs = ((0, 7), (1, 2), (3, 4), (5, 6))

    def rows_of(source):
        return weights[pl.ds(pl.multiple_of(source * HALF, HALF), HALF), :]

    for g in range(4):
        acc = jnp.zeros((part, 2 * HALF), F32)
        for m, n in pairs:
            h = jnp.concatenate([chunks[k][g * part : (g + 1) * part, :] for k in (m, n)], axis=1)
            w = jnp.concatenate([rows_of(sources[m]), rows_of(sources[n])], axis=0)
            acc = acc + jnp.dot(h, w, preferred_element_type=F32)
        to_slabs(acc, out, 8 * g)


def combine_kernel(rows, gains, returned, mixture):
    n_tok = rows.shape[0]
    slabs, part = 8 * SLAB, 8 * CAP
    sums = [jnp.zeros((n_tok, 2 * HALF), F32) for _ in range(2)]
    for g in range(returned.shape[0] // slabs):
        left, right = from_slabs(returned[g * slabs : (g + 1) * slabs, :])
        both = jnp.concatenate([left, right], axis=1)
        ids = lax.broadcasted_iota(jnp.int32, (n_tok, part), 1) + g * part
        for k in range(2):
            onehot = (ids == rows[:, k : k + 1]).astype(F32).astype(BF16)
            sums[k] = sums[k] + jnp.dot(onehot, both, preferred_element_type=F32)
    mixture[...] = (gains[:, 0:1] * sums[0] + gains[:, 1:2] * sums[1]).astype(BF16)


LIMIT = pltpu.CompilerParams(vmem_limit_bytes=16 * 1024 * 1024)


def in_vmem(*arrays):
    return [pltpu.with_memory_space_constraint(x, pltpu.VMEM) for x in arrays]


def all_to_all(x):
    return lax.all_to_all(x, "fs", split_axis=0, concat_axis=0, tiled=True)


def ring(x, last):
    n = lax.axis_size("tp")

    def step(v, side):
        shift = 1 if side == "r" else -1
        return lax.ppermute(v, "tp", [(d, (d + shift) % n) for d in range(n)])

    r1, l1 = step(x, "r"), step(x, "l")
    r2, l2 = step(r1, "r"), step(l1, "l")
    r3, l3 = step(r2, "r"), step(l2, "l")
    x4 = step(r3, "r") if last == "r" else step(l3, "l")
    return (x, r1, l1, r2, l2, r3, l3, x4)


def mixture_of_experts(tokens, norm_gain, gate_weight, up_weight, down_weight, routes, route_weights):
    experts, _, cols = gate_weight.shape
    n_tok = tokens.shape[0]
    me = lax.axis_index("tp").reshape(1).astype(jnp.int32)
    smem = pl.BlockSpec(memory_space=pltpu.SMEM)
    vmem = pl.BlockSpec(memory_space=pltpu.VMEM)
    slabs = (experts, SLAB, HALF)
    outbound, rows = pl.pallas_call(
        route_kernel,
        in_specs=[vmem, vmem],
        out_specs=(vmem, vmem),
        out_shape=(pltpu.VMEM(slabs, BF16), pltpu.VMEM((8, n_tok), jnp.int32)),
        name="route",
        compiler_params=LIMIT,
    )(*in_vmem(routes.T, tokens))
    arrived = all_to_all(outbound).reshape(experts * SLAB, HALF)
    gain = norm_gain[None, :, None]
    both_low = jnp.concatenate([gain * gate_weight, gain * up_weight], axis=2).astype(BF16)
    both_serve = all_to_all(both_low).reshape(-1, 2 * cols)
    cut = experts * SLAB // 2
    halves = ring(arrived[:cut], "r") + ring(arrived[cut:], "l")
    hidden = pl.pallas_call(
        ffn_kernel,
        in_specs=[smem] + [vmem] * 17,
        out_specs=vmem,
        out_shape=pltpu.VMEM((experts * CAP, cols), BF16),
        name="ffn",
        compiler_params=LIMIT,
    )(me, *in_vmem(*halves, both_serve))
    down_low = down_weight.astype(BF16)
    down_serve = all_to_all(down_low).reshape(-1, down_low.shape[2])
    expert_out = pl.pallas_call(
        down_kernel,
        in_specs=[smem] + [vmem] * 9,
        out_specs=vmem,
        out_shape=pltpu.VMEM(slabs, BF16),
        name="down",
        compiler_params=LIMIT,
    )(me, *in_vmem(*ring(hidden, "r"), down_serve))
    returned = all_to_all(expert_out).reshape(experts * SLAB, HALF)
    mixture = pl.pallas_call(
        combine_kernel,
        in_specs=[vmem] * 3,
        out_specs=vmem,
        out_shape=jax.ShapeDtypeStruct(tokens.shape, BF16),
        name="combine",
        compiler_params=LIMIT,
    )(*in_vmem(rows.T, route_weights, returned))
    gate_serve, up_serve = both_serve[None, :, :cols], both_serve[None, :, cols:]
    return (gate_serve, up_serve, down_serve[None], mixture)


def solution(mesh):
    block = ("grp", "fs")
    return jax.shard_map(
        mixture_of_experts,
        mesh=mesh,
        in_specs=(
            P(block, "tp"),
            P("fs"),
            P(None, "fs", "tp"),
            P(None, "fs", "tp"),
            P(None, "fs", "tp"),
            P(block, None),
            P(block, None),
        ),
        out_specs=(
            P(block, None, "tp"),
            P(block, None, "tp"),
            P(block, None, "tp"),
            P(block, "tp"),
        ),
        check_vma=False,
    )
```

```python
import jax
import jax.numpy as jnp
from jax import lax
from jax.experimental import pallas as pl
from jax.experimental.pallas import tpu as pltpu
from jax.sharding import PartitionSpec as P


CAP = 36
MAIN = 32
SLAB = 72
HALF = 128
BF16 = jnp.bfloat16
F32 = jnp.float32
epsilon = 1e-06


def tile_row(shape):
    return lax.broadcasted_iota(jnp.int32, shape, len(shape) - 2)


def from_slabs(x):
    x = x.reshape(8, SLAB, HALF)
    left = x[:, :MAIN].reshape(8 * MAIN, HALF)
    right = x[:, MAIN : 2 * MAIN].reshape(8 * MAIN, HALF)
    rest = x[:, 2 * MAIN :].astype(F32).reshape(4, 2, 8, HALF)
    even, odd = rest[:, 0], rest[:, 1]
    low = tile_row((4, 8, HALF)) < CAP - MAIN
    rest_l = jnp.where(low, even, pltpu.roll(odd, 4, 1)).reshape(32, HALF).astype(BF16)
    rest_r = jnp.where(low, pltpu.roll(even, 4, 1), odd).reshape(32, HALF).astype(BF16)
    return jnp.concatenate([left, rest_l], axis=0), jnp.concatenate([right, rest_r], axis=0)


def to_slabs(rows, out, first):
    pairs = 8 * MAIN
    rest_l = rows[pairs:, :HALF].reshape(4, 8, HALF)
    rest_r = rows[pairs:, HALF:].reshape(4, 8, HALF)
    low = tile_row((4, 8, HALF)) < CAP - MAIN
    even = jnp.where(low, rest_l, pltpu.roll(rest_r, 4, 1))
    odd = jnp.where(low, pltpu.roll(rest_l, 4, 1), rest_r)
    rest = jnp.stack([even, odd], axis=1).reshape(8, 8, HALF)
    out[first : first + 8, 0:MAIN, :] = rows[:pairs, :HALF].reshape(8, MAIN, HALF).astype(BF16)
    out[first : first + 8, MAIN : 2 * MAIN, :] = rows[:pairs, HALF:].reshape(8, MAIN, HALF).astype(BF16)
    out[first : first + 8, 2 * MAIN :, :] = rest.astype(BF16)


def route_kernel(routes, tokens, outbound, rows):
    experts = outbound.shape[0]
    n_tok = tokens.shape[0]
    first, second = routes[0:1, :], routes[1:2, :]
    ids = lax.broadcasted_iota(jnp.int32, (experts, n_tok), 0)
    hit0 = (ids == first).astype(F32)
    hit1 = (ids == second).astype(F32)
    before = (
        lax.broadcasted_iota(jnp.int32, (n_tok, n_tok), 0)
        < lax.broadcasted_iota(jnp.int32, (n_tok, n_tok), 1)
    ).astype(F32).astype(BF16)
    count0 = jnp.dot(hit0.astype(BF16), before, preferred_element_type=F32)
    count1 = jnp.dot(hit1.astype(BF16), before, preferred_element_type=F32)
    count1 = count1 + jnp.sum(hit0, axis=1, keepdims=True)

    def row_of(expert, hit, count):
        slot = jnp.sum(hit * count, axis=0, keepdims=True).astype(jnp.int32)
        base = jnp.right_shift(expert, 3) * (8 * CAP)
        within = jnp.bitwise_and(expert, 7)
        main = within * MAIN + slot
        rest = 8 * MAIN + within * (CAP - MAIN) + (slot - MAIN)
        return base + jnp.where(slot < MAIN, main, rest)

    row0, row1 = row_of(first, hit0, count0), row_of(second, hit1, count1)
    rows[...] = jnp.concatenate([row0, row1] * 4, axis=0)
    part = 8 * CAP
    for g in range(experts // 8):
        ids = lax.broadcasted_iota(jnp.int32, (part, n_tok), 0) + g * part
        select = jnp.logical_or(ids == row0, ids == row1).astype(F32).astype(BF16)
        out = jnp.dot(select, tokens[...], preferred_element_type=F32)
        to_slabs(out, outbound, 8 * g)


def offsets_of(me):
    n_tp = 8
    return [(me + offset + n_tp) % n_tp for offset in (0, -1, 1, -2, 2, -3, 3, 4)]


def join_pieces(mine, pieces, serve):
    count, rows = len(pieces), pieces[0].shape[1]
    for n, piece in enumerate(pieces):
        place = (mine + n) % count
        serve[:, pl.ds(pl.multiple_of(place * rows, rows), rows), :] = piece[...]


def ffn_kernel(me, *refs):
    chunks, pieces = refs[0:16], refs[16:-5]
    hidden, serve, held, chunk_done, piece_done = refs[-5:]
    sources = offsets_of(me[0])
    features = serve.shape[0] * serve.shape[1]
    count, rows = len(pieces), pieces[0].shape[1]
    spread = 2 * HALF // serve.shape[1]
    part, slabs = 8 * CAP, 8 * SLAB

    def fetch_piece(n):
        place = (me[1] + n) % count
        target = serve.at[:, pl.ds(pl.multiple_of(place * rows, rows), rows), :]
        return pltpu.make_async_copy(pieces[n], target, piece_done.at[n])

    def fetch(g, k):
        n = 8 * (g // 2) + k
        span = pl.ds((g % 2) * slabs, slabs)
        return pltpu.make_async_copy(chunks[n].at[span, :], held.at[g, k], chunk_done.at[g, k])

    for n in range(count):
        fetch_piece(n).start()
    for g in range(4):
        for k in range(8):
            fetch(g, k).start()
    for n in range(count):
        fetch_piece(n).wait()
    for g in range(4):
        acc = jnp.zeros((part, 2 * HALF), F32)
        square = jnp.zeros((part, HALF), F32)
        for k, source in enumerate(sources):
            fetch(g, k).wait()
            left, right = from_slabs(held[g, k])
            w = serve[pl.ds(source * spread, spread)].reshape(2 * HALF, 2 * HALF)
            both = jnp.concatenate([left, right], axis=1)
            acc = acc + jnp.dot(both, w, preferred_element_type=F32)
            l32, r32 = left.astype(F32), right.astype(F32)
            square = square + (l32 * l32 + r32 * r32)
        total = jnp.sum(square, axis=1, keepdims=True)
        scale = lax.rsqrt(total * (1.0 / features) + epsilon)
        gate = acc[:, :HALF] * scale
        up = acc[:, HALF:] * scale
        value = gate / (1.0 + jnp.exp(-gate)) * up
        hidden[g * part : (g + 1) * part, :] = value.astype(BF16)


def down_kernel(me, *refs):
    chunks, pieces, out, serve_out, serve, done = refs[0:8], refs[8:-4], *refs[-4:]
    sources = offsets_of(me[0])
    join_pieces(me[1], pieces, serve)
    copy = pltpu.make_async_copy(serve, serve_out, done)
    copy.start()
    spread = HALF // serve.shape[1]
    part = 8 * CAP
    pairs = ((0, 7), (1, 2), (3, 4), (5, 6))

    def rows_of(source):
        return serve[pl.ds(source * spread, spread)].reshape(HALF, 2 * HALF)

    for g in range(4):
        acc = jnp.zeros((part, 2 * HALF), F32)
        for m, n in pairs:
            h = jnp.concatenate([chunks[k][g * part : (g + 1) * part, :] for k in (m, n)], axis=1)
            w = jnp.concatenate([rows_of(sources[m]), rows_of(sources[n])], axis=0)
            acc = acc + jnp.dot(h, w, preferred_element_type=F32)
        to_slabs(acc, out, 8 * g)
    copy.wait()


def combine_kernel(rows, gains, returned, mixture):
    n_tok = rows.shape[0]
    slabs, part = 8 * SLAB, 8 * CAP
    sums = [jnp.zeros((n_tok, 2 * HALF), F32) for _ in range(2)]
    for g in range(returned.shape[0] // slabs):
        left, right = from_slabs(returned[g * slabs : (g + 1) * slabs, :])
        both = jnp.concatenate([left, right], axis=1)
        ids = lax.broadcasted_iota(jnp.int32, (n_tok, part), 1) + g * part
        for k in range(2):
            onehot = (ids == rows[:, k : k + 1]).astype(F32).astype(BF16)
            sums[k] = sums[k] + jnp.dot(onehot, both, preferred_element_type=F32)
    mixture[...] = (gains[:, 0:1] * sums[0] + gains[:, 1:2] * sums[1]).astype(BF16)


LIMIT = pltpu.CompilerParams(vmem_limit_bytes=16 * 1024 * 1024)


def in_vmem(*arrays):
    return [pltpu.with_memory_space_constraint(x, pltpu.VMEM) for x in arrays]


def in_hbm(*arrays):
    return [pltpu.with_memory_space_constraint(x, pltpu.HBM) for x in arrays]


def all_to_all(x):
    return lax.all_to_all(x, "fs", split_axis=0, concat_axis=0, tiled=True)


def ring(x, last):
    n = lax.axis_size("tp")

    def step(v, side):
        shift = 1 if side == "r" else -1
        return lax.ppermute(v, "tp", [(d, (d + shift) % n) for d in range(n)])

    r1, l1 = step(x, "r"), step(x, "l")
    r2, l2 = step(r1, "r"), step(l1, "l")
    r3, l3 = step(r2, "r"), step(l2, "l")
    x4 = step(r3, "r") if last == "r" else step(l3, "l")
    return (x, r1, l1, r2, l2, r3, l3, x4)


def mixture_of_experts(tokens, norm_gain, gate_weight, up_weight, down_weight, routes, route_weights):
    experts, rows_in, cols = gate_weight.shape
    rows_down, down_cols = down_weight.shape[1:]
    n_tok = tokens.shape[0]
    groups = lax.axis_size("grp")
    count = 2 if groups % 2 == 0 else 1
    mine = lax.axis_index("grp") % count
    me = jnp.stack([lax.axis_index("tp"), mine]).astype(jnp.int32)
    smem = pl.BlockSpec(memory_space=pltpu.SMEM)
    vmem = pl.BlockSpec(memory_space=pltpu.VMEM)
    slabs = (experts, SLAB, HALF)
    outbound, rows = pl.pallas_call(
        route_kernel,
        in_specs=[vmem, vmem],
        out_specs=(vmem, vmem),
        out_shape=(pltpu.VMEM(slabs, BF16), pltpu.VMEM((8, n_tok), jnp.int32)),
        name="route",
        compiler_params=LIMIT,
    )(routes.T, tokens)
    arrived = all_to_all(outbound).reshape(experts * SLAB, HALF)

    def piece(x, axis):
        size = x.shape[axis] // count
        return lax.dynamic_slice_in_dim(x, mine * size, size, axis)

    def swapped(x):
        if count == 1:
            return [x]
        return [x, lax.ppermute(x, "grp", [(g, g ^ 1) for g in range(groups)])]

    gain = piece(norm_gain, 0)[None, :, None]
    both_low = jnp.concatenate([gain * piece(gate_weight, 1), gain * piece(up_weight, 1)], axis=2)
    weights_low = jnp.concatenate([both_low, piece(down_weight, 1)], axis=1).astype(BF16)
    arrived_weights = all_to_all(weights_low)
    both_pieces = swapped(arrived_weights[:, : rows_in // count])
    down_pieces = swapped(arrived_weights[:, rows_in // count :])
    cut = experts * SLAB // 2
    halves = ring(arrived[:cut], "r") + ring(arrived[cut:], "l")
    hidden, both_serve = pl.pallas_call(
        ffn_kernel,
        in_specs=[smem] + [pl.BlockSpec(memory_space=pl.ANY)] * (16 + count),
        out_specs=(vmem, vmem),
        out_shape=(
            pltpu.VMEM((experts * CAP, cols), BF16),
            pltpu.VMEM((experts, rows_in, 2 * cols), BF16),
        ),
        scratch_shapes=[
            pltpu.VMEM((4, 8, 8 * SLAB, HALF), BF16),
            pltpu.SemaphoreType.DMA((4, 8)),
            pltpu.SemaphoreType.DMA((count,)),
        ],
        name="ffn",
        compiler_params=LIMIT,
    )(me, *in_hbm(*halves, *both_pieces))
    expert_out, down_serve = pl.pallas_call(
        down_kernel,
        in_specs=[smem] + [vmem] * (8 + count),
        out_specs=(vmem, pl.BlockSpec(memory_space=pl.ANY)),
        out_shape=(
            pltpu.VMEM(slabs, BF16),
            jax.ShapeDtypeStruct((experts, rows_down, down_cols), BF16),
        ),
        scratch_shapes=[
            pltpu.VMEM((experts, rows_down, down_cols), BF16),
            pltpu.SemaphoreType.DMA,
        ],
        name="down",
        compiler_params=LIMIT,
    )(me, *in_vmem(*ring(hidden, "r"), *down_pieces))
    returned = all_to_all(expert_out).reshape(experts * SLAB, HALF)
    mixture = pl.pallas_call(
        combine_kernel,
        in_specs=[vmem] * 3,
        out_specs=vmem,
        out_shape=jax.ShapeDtypeStruct(tokens.shape, BF16),
        name="combine",
        compiler_params=LIMIT,
    )(*in_vmem(rows.T, route_weights, returned))
    both_serve = both_serve.reshape(1, -1, 2 * cols)
    gate_serve, up_serve = both_serve[:, :, :cols], both_serve[:, :, cols:]
    return (gate_serve, up_serve, down_serve.reshape(1, -1, down_cols), mixture)


def solution(mesh):
    block = ("grp", "fs")
    return jax.shard_map(
        mixture_of_experts,
        mesh=mesh,
        in_specs=(
            P(block, "tp"),
            P("fs"),
            P(None, "fs", "tp"),
            P(None, "fs", "tp"),
            P(None, "fs", "tp"),
            P(block, None),
            P(block, None),
        ),
        out_specs=(
            P(block, None, "tp"),
            P(block, None, "tp"),
            P(block, None, "tp"),
            P(block, "tp"),
        ),
        check_vma=False,
    )
```

```python
import jax
import jax.numpy as jnp
from jax import lax
from jax.experimental import pallas as pl
from jax.experimental.pallas import tpu as pltpu
from jax.sharding import PartitionSpec as P


CAP = 36
MAIN = 32
SLAB = 72
HALF = 128
BF16 = jnp.bfloat16
F32 = jnp.float32
epsilon = 1e-06


def tile_row(shape):
    return lax.broadcasted_iota(jnp.int32, shape, len(shape) - 2)


def from_slabs(x):
    x = x.reshape(8, SLAB, HALF)
    left = x[:, :MAIN].reshape(8 * MAIN, HALF)
    right = x[:, MAIN : 2 * MAIN].reshape(8 * MAIN, HALF)
    rest = x[:, 2 * MAIN :].astype(F32).reshape(4, 2, 8, HALF)
    even, odd = rest[:, 0], rest[:, 1]
    low = tile_row((4, 8, HALF)) < CAP - MAIN
    rest_l = jnp.where(low, even, pltpu.roll(odd, 4, 1)).reshape(32, HALF).astype(BF16)
    rest_r = jnp.where(low, pltpu.roll(even, 4, 1), odd).reshape(32, HALF).astype(BF16)
    return jnp.concatenate([left, rest_l], axis=0), jnp.concatenate([right, rest_r], axis=0)


def to_slabs(rows, out, first):
    pairs = 8 * MAIN
    rest_l = rows[pairs:, :HALF].reshape(4, 8, HALF)
    rest_r = rows[pairs:, HALF:].reshape(4, 8, HALF)
    low = tile_row((4, 8, HALF)) < CAP - MAIN
    even = jnp.where(low, rest_l, pltpu.roll(rest_r, 4, 1))
    odd = jnp.where(low, pltpu.roll(rest_l, 4, 1), rest_r)
    rest = jnp.stack([even, odd], axis=1).reshape(8, 8, HALF)
    out[first : first + 8, 0:MAIN, :] = rows[:pairs, :HALF].reshape(8, MAIN, HALF).astype(BF16)
    out[first : first + 8, MAIN : 2 * MAIN, :] = rows[:pairs, HALF:].reshape(8, MAIN, HALF).astype(BF16)
    out[first : first + 8, 2 * MAIN :, :] = rest.astype(BF16)


def route_kernel(routes_in, tokens_in, outbound, rows, routes, tokens, done):
    experts = outbound.shape[0]
    n_tok = tokens.shape[0]
    fetch_routes = pltpu.make_async_copy(routes_in, routes, done.at[0])
    fetch_tokens = pltpu.make_async_copy(tokens_in, tokens, done.at[1])
    fetch_routes.start()
    fetch_tokens.start()
    fetch_routes.wait()
    first, second = routes[0:1, :], routes[1:2, :]
    ids = lax.broadcasted_iota(jnp.int32, (experts, n_tok), 0)
    hit0 = (ids == first).astype(F32)
    hit1 = (ids == second).astype(F32)
    before = (
        lax.broadcasted_iota(jnp.int32, (n_tok, n_tok), 0)
        < lax.broadcasted_iota(jnp.int32, (n_tok, n_tok), 1)
    ).astype(F32).astype(BF16)
    count0 = jnp.dot(hit0.astype(BF16), before, preferred_element_type=F32)
    count1 = jnp.dot(hit1.astype(BF16), before, preferred_element_type=F32)
    count1 = count1 + jnp.sum(hit0, axis=1, keepdims=True)

    def row_of(expert, hit, count):
        slot = jnp.sum(hit * count, axis=0, keepdims=True).astype(jnp.int32)
        base = jnp.right_shift(expert, 3) * (8 * CAP)
        within = jnp.bitwise_and(expert, 7)
        main = within * MAIN + slot
        rest = 8 * MAIN + within * (CAP - MAIN) + (slot - MAIN)
        return base + jnp.where(slot < MAIN, main, rest)

    row0, row1 = row_of(first, hit0, count0), row_of(second, hit1, count1)
    rows[...] = jnp.concatenate([row0, row1] * 4, axis=0)
    part = 8 * CAP
    fetch_tokens.wait()
    for g in range(experts // 8):
        ids = lax.broadcasted_iota(jnp.int32, (part, n_tok), 0) + g * part
        select = jnp.logical_or(ids == row0, ids == row1).astype(F32).astype(BF16)
        out = jnp.dot(select, tokens[...], preferred_element_type=F32)
        to_slabs(out, outbound, 8 * g)


def offsets_of(me):
    n_tp = 8
    return [(me + offset + n_tp) % n_tp for offset in (0, -1, 1, -2, 2, -3, 3, 4)]


def join_pieces(mine, pieces, serve):
    count, rows = len(pieces), pieces[0].shape[1]
    for n, piece in enumerate(pieces):
        place = (mine + n) % count
        serve[:, pl.ds(pl.multiple_of(place * rows, rows), rows), :] = piece[...]


def ffn_kernel(me, *refs):
    whole, middle, late, pieces = refs[0:3], (refs[3:5], refs[5:7]), (refs[7:10], refs[10:13]), refs[13:-4]
    hidden, serve, held, done = refs[-4:]
    own, r1, l1, r2, l2, r3, l3, x4 = offsets_of(me[0])
    features = serve.shape[0] * serve.shape[1]
    spread = 2 * HALF // serve.shape[1]
    part, slabs = 8 * CAP, 8 * SLAB

    def fetch(g, k):
        if k < 3:
            source = whole[k].at[pl.ds(g * slabs, slabs), :]
        else:
            source = middle[g // 2][k - 3].at[pl.ds((g % 2) * slabs, slabs), :]
        return pltpu.make_async_copy(source, held.at[g, k], done.at[g, k])

    for g in range(4):
        for k in range(5):
            fetch(g, k).start()
    join_pieces(me[1], pieces, serve)
    for g in range(4):
        acc = jnp.zeros((part, 2 * HALF), F32)
        square = jnp.zeros((part, HALF), F32)
        for k, source in enumerate((r3, l3, x4, own, r1, l1, r2, l2)):
            if k < 3:
                x = late[g // 2][k][(g % 2) * slabs : (g % 2 + 1) * slabs, :]
            else:
                fetch(g, k - 3).wait()
                x = held[g, k - 3]
            left, right = from_slabs(x)
            w = serve[pl.ds(source * spread, spread)].reshape(2 * HALF, 2 * HALF)
            both = jnp.concatenate([left, right], axis=1)
            acc = acc + jnp.dot(both, w, preferred_element_type=F32)
            l32, r32 = left.astype(F32), right.astype(F32)
            square = square + (l32 * l32 + r32 * r32)
        total = jnp.sum(square, axis=1, keepdims=True)
        scale = lax.rsqrt(total * (1.0 / features) + epsilon)
        gate = acc[:, :HALF] * scale
        up = acc[:, HALF:] * scale
        value = gate / (1.0 + jnp.exp(-gate)) * up
        hidden[g * part : (g + 1) * part, :] = value.astype(BF16)


def down_kernel(me, *refs):
    chunks, pieces, out, serve = refs[0:8], refs[8:-2], *refs[-2:]
    sources = offsets_of(me[0])
    join_pieces(me[1], pieces, serve)
    spread = HALF // serve.shape[1]
    part = 8 * CAP
    pairs = ((0, 7), (1, 2), (3, 4), (5, 6))

    def rows_of(source):
        return serve[pl.ds(source * spread, spread)].reshape(HALF, 2 * HALF)

    for g in range(4):
        acc = jnp.zeros((part, 2 * HALF), F32)
        for m, n in pairs:
            h = jnp.concatenate([chunks[k][g * part : (g + 1) * part, :] for k in (m, n)], axis=1)
            w = jnp.concatenate([rows_of(sources[m]), rows_of(sources[n])], axis=0)
            acc = acc + jnp.dot(h, w, preferred_element_type=F32)
        to_slabs(acc, out, 8 * g)


def combine_kernel(rows, gains, returned, mixture):
    n_tok = rows.shape[0]
    slabs, part = 8 * SLAB, 8 * CAP
    sums = [jnp.zeros((n_tok, 2 * HALF), F32) for _ in range(2)]
    for g in range(returned.shape[0] // slabs):
        left, right = from_slabs(returned[g * slabs : (g + 1) * slabs, :])
        both = jnp.concatenate([left, right], axis=1)
        ids = lax.broadcasted_iota(jnp.int32, (n_tok, part), 1) + g * part
        for k in range(2):
            onehot = (ids == rows[:, k : k + 1]).astype(F32).astype(BF16)
            sums[k] = sums[k] + jnp.dot(onehot, both, preferred_element_type=F32)
    mixture[...] = (gains[:, 0:1] * sums[0] + gains[:, 1:2] * sums[1]).astype(BF16)


LIMIT = pltpu.CompilerParams(vmem_limit_bytes=16 * 1024 * 1024)


def in_vmem(*arrays):
    return [pltpu.with_memory_space_constraint(x, pltpu.VMEM) for x in arrays]


def in_hbm(*arrays):
    return [pltpu.with_memory_space_constraint(x, pltpu.HBM) for x in arrays]


def all_to_all(x):
    return lax.all_to_all(x, "fs", split_axis=0, concat_axis=0, tiled=True)


def step(x, shift):
    n = lax.axis_size("tp")
    return lax.ppermute(x, "tp", [(d, (d + shift) % n) for d in range(n)])


def ring(x):
    r1, l1 = step(x, 1), step(x, -1)
    r2, l2 = step(r1, 1), step(l1, -1)
    r3, l3 = step(r2, 1), step(l2, -1)
    return (x, r1, l1, r2, l2, r3, l3, step(r3, 1))


def token_ring(x):
    cut = x.shape[0] // 2
    r1, l1 = step(x, 1), step(x, -1)
    middle, late = [], []
    for span, end in ((slice(0, cut), "r"), (slice(cut, None), "l")):
        r2, l2 = step(r1[span], 1), step(l1[span], -1)
        r3, l3 = step(r2, 1), step(l2, -1)
        x4 = step(r3, 1) if end == "r" else step(l3, -1)
        middle += [r2, l2]
        late += [r3, l3, x4]
    return (x, r1, l1), middle, late


def mixture_of_experts(tokens, norm_gain, gate_weight, up_weight, down_weight, routes, route_weights):
    experts, rows_in, cols = gate_weight.shape
    rows_down, down_cols = down_weight.shape[1:]
    n_tok = tokens.shape[0]
    groups = lax.axis_size("grp")
    count = 2 if groups % 2 == 0 else 1
    mine = lax.axis_index("grp") % count
    me = jnp.stack([lax.axis_index("tp"), mine]).astype(jnp.int32)
    smem = pl.BlockSpec(memory_space=pltpu.SMEM)
    vmem = pl.BlockSpec(memory_space=pltpu.VMEM)
    anywhere = pl.BlockSpec(memory_space=pl.ANY)
    slabs = (experts, SLAB, HALF)
    outbound, rows = pl.pallas_call(
        route_kernel,
        in_specs=[anywhere, anywhere],
        out_specs=(vmem, vmem),
        scratch_shapes=[
            pltpu.VMEM((2, n_tok), jnp.int32),
            pltpu.VMEM(tokens.shape, BF16),
            pltpu.SemaphoreType.DMA((2,)),
        ],
        out_shape=(pltpu.VMEM(slabs, BF16), pltpu.VMEM((8, n_tok), jnp.int32)),
        name="route",
        compiler_params=LIMIT,
    )(*in_hbm(routes.T, tokens))
    arrived = all_to_all(outbound).reshape(experts * SLAB, HALF)

    def piece(x, axis):
        size = x.shape[axis] // count
        return lax.dynamic_slice_in_dim(x, mine * size, size, axis)

    def swapped(x):
        if count == 1:
            return [x]
        return [x, lax.ppermute(x, "grp", [(g, g ^ 1) for g in range(groups)])]

    gain = piece(norm_gain, 0)[None, :, None]
    both_low = jnp.concatenate([gain * piece(gate_weight, 1), gain * piece(up_weight, 1)], axis=2)
    weights_low = jnp.concatenate([both_low, piece(down_weight, 1)], axis=1).astype(BF16)
    arrived_weights = all_to_all(weights_low)
    both_pieces = swapped(arrived_weights[:, : rows_in // count])
    down_pieces = swapped(arrived_weights[:, rows_in // count :])
    whole, middle, late = token_ring(arrived)
    hidden = pl.pallas_call(
        ffn_kernel,
        in_specs=[smem] + [anywhere] * 7 + [vmem] * (6 + count),
        out_specs=vmem,
        out_shape=pltpu.VMEM((experts * CAP, cols), BF16),
        scratch_shapes=[
            pltpu.VMEM((experts, rows_in, 2 * cols), BF16),
            pltpu.VMEM((4, 5, 8 * SLAB, HALF), BF16),
            pltpu.SemaphoreType.DMA((4, 5)),
        ],
        name="ffn",
        compiler_params=LIMIT,
    )(me, *in_hbm(*whole, *middle), *in_vmem(*late, *both_pieces))
    expert_out = pl.pallas_call(
        down_kernel,
        in_specs=[smem] + [vmem] * (8 + count),
        out_specs=vmem,
        out_shape=pltpu.VMEM(slabs, BF16),
        scratch_shapes=[pltpu.VMEM((experts, rows_down, down_cols), BF16)],
        name="down",
        compiler_params=LIMIT,
    )(me, *in_vmem(*ring(hidden), *down_pieces))
    returned = all_to_all(expert_out).reshape(experts * SLAB, HALF)
    mixture = pl.pallas_call(
        combine_kernel,
        in_specs=[vmem] * 3,
        out_specs=vmem,
        out_shape=jax.ShapeDtypeStruct(tokens.shape, BF16),
        name="combine",
        compiler_params=LIMIT,
    )(*in_vmem(rows.T, route_weights, returned))

    def assembled(pieces):
        if count == 1:
            return pieces[0].reshape(1, -1, pieces[0].shape[2])
        own, other = pieces
        both = jnp.where(mine == 0, own, other), jnp.where(mine == 0, other, own)
        return jnp.concatenate(both, axis=1).reshape(1, -1, own.shape[2])

    gate_serve = assembled([x[:, :, :cols] for x in both_pieces])
    up_serve = assembled([x[:, :, cols:] for x in both_pieces])
    return (gate_serve, up_serve, assembled(down_pieces), mixture)


def solution(mesh):
    block = ("grp", "fs")
    return jax.shard_map(
        mixture_of_experts,
        mesh=mesh,
        in_specs=(
            P(block, "tp"),
            P("fs"),
            P(None, "fs", "tp"),
            P(None, "fs", "tp"),
            P(None, "fs", "tp"),
            P(block, None),
            P(block, None),
        ),
        out_specs=(
            P(block, None, "tp"),
            P(block, None, "tp"),
            P(block, None, "tp"),
            P(block, "tp"),
        ),
        check_vma=False,
    )
```

```python
import jax
import jax.numpy as jnp
from jax import lax
from jax.experimental import pallas as pl
from jax.experimental.pallas import tpu as pltpu
from jax.sharding import PartitionSpec as P


CAP = 36
FETCHED = (0,)
MAIN = 32
SLAB = 72
HALF = 128
BF16 = jnp.bfloat16
F32 = jnp.float32
epsilon = 1e-06


def tile_row(shape):
    return lax.broadcasted_iota(jnp.int32, shape, len(shape) - 2)


def from_slabs(x):
    x = x.reshape(8, SLAB, HALF)
    left = x[:, :MAIN].reshape(8 * MAIN, HALF)
    right = x[:, MAIN : 2 * MAIN].reshape(8 * MAIN, HALF)
    rest = x[:, 2 * MAIN :].astype(F32).reshape(4, 2, 8, HALF)
    even, odd = rest[:, 0], rest[:, 1]
    low = tile_row((4, 8, HALF)) < CAP - MAIN
    rest_l = jnp.where(low, even, pltpu.roll(odd, 4, 1)).reshape(32, HALF).astype(BF16)
    rest_r = jnp.where(low, pltpu.roll(even, 4, 1), odd).reshape(32, HALF).astype(BF16)
    return jnp.concatenate([left, rest_l], axis=0), jnp.concatenate([right, rest_r], axis=0)


def to_slabs(rows, out, first):
    pairs = 8 * MAIN
    rest_l = rows[pairs:, :HALF].reshape(4, 8, HALF)
    rest_r = rows[pairs:, HALF:].reshape(4, 8, HALF)
    low = tile_row((4, 8, HALF)) < CAP - MAIN
    even = jnp.where(low, rest_l, pltpu.roll(rest_r, 4, 1))
    odd = jnp.where(low, pltpu.roll(rest_l, 4, 1), rest_r)
    rest = jnp.stack([even, odd], axis=1).reshape(8, 8, HALF)
    out[first : first + 8, 0:MAIN, :] = rows[:pairs, :HALF].reshape(8, MAIN, HALF).astype(BF16)
    out[first : first + 8, MAIN : 2 * MAIN, :] = rows[:pairs, HALF:].reshape(8, MAIN, HALF).astype(BF16)
    out[first : first + 8, 2 * MAIN :, :] = rest.astype(BF16)


def route_kernel(routes_in, tokens_in, outbound, rows, routes, tokens, done):
    experts = outbound.shape[0]
    n_tok = tokens.shape[0]
    fetch_routes = pltpu.make_async_copy(routes_in, routes, done.at[0])
    fetch_tokens = pltpu.make_async_copy(tokens_in, tokens, done.at[1])
    fetch_routes.start()
    fetch_tokens.start()
    fetch_routes.wait()
    first, second = routes[0:1, :], routes[1:2, :]
    ids = lax.broadcasted_iota(jnp.int32, (experts, n_tok), 0)
    hit0 = (ids == first).astype(F32)
    hit1 = (ids == second).astype(F32)
    before = (
        lax.broadcasted_iota(jnp.int32, (n_tok, n_tok), 0)
        < lax.broadcasted_iota(jnp.int32, (n_tok, n_tok), 1)
    ).astype(F32).astype(BF16)
    count0 = jnp.dot(hit0.astype(BF16), before, preferred_element_type=F32)
    count1 = jnp.dot(hit1.astype(BF16), before, preferred_element_type=F32)
    count1 = count1 + jnp.sum(hit0, axis=1, keepdims=True)

    def row_of(expert, hit, count):
        slot = jnp.sum(hit * count, axis=0, keepdims=True).astype(jnp.int32)
        base = jnp.right_shift(expert, 3) * (8 * CAP)
        within = jnp.bitwise_and(expert, 7)
        main = within * MAIN + slot
        rest = 8 * MAIN + within * (CAP - MAIN) + (slot - MAIN)
        return base + jnp.where(slot < MAIN, main, rest)

    row0, row1 = row_of(first, hit0, count0), row_of(second, hit1, count1)
    rows[...] = jnp.concatenate([row0, row1] * 4, axis=0)
    part = 8 * CAP
    fetch_tokens.wait()
    for g in range(experts // 8):
        ids = lax.broadcasted_iota(jnp.int32, (part, n_tok), 0) + g * part
        select = jnp.logical_or(ids == row0, ids == row1).astype(F32).astype(BF16)
        out = jnp.dot(select, tokens[...], preferred_element_type=F32)
        to_slabs(out, outbound, 8 * g)


def offsets_of(me):
    n_tp = 8
    return [(me + offset + n_tp) % n_tp for offset in (0, -1, 1, -2, 2, -3, 3, 4)]


def join_pieces(mine, pieces, serve):
    count, rows = len(pieces), pieces[0].shape[1]
    for n, piece in enumerate(pieces):
        place = (mine + n) % count
        serve[:, pl.ds(pl.multiple_of(place * rows, rows), rows), :] = piece[...]


def ffn_kernel(me, *refs):
    chunks, pieces = (refs[0:8], refs[8:16]), refs[16:-4]
    hidden, serve, held, done = refs[-4:]
    sources = offsets_of(me[0])
    features = serve.shape[0] * serve.shape[1]
    spread = 2 * HALF // serve.shape[1]
    part, slabs = 8 * CAP, 8 * SLAB

    def fetch(g, n):
        source = chunks[g // 2][FETCHED[n]].at[pl.ds((g % 2) * slabs, slabs), :]
        return pltpu.make_async_copy(source, held.at[g, n], done.at[g, n])

    for g in range(4):
        for n in range(len(FETCHED)):
            fetch(g, n).start()
    join_pieces(me[1], pieces, serve)
    order = [k for k in range(8) if k not in FETCHED] + list(FETCHED)
    for g in range(4):
        acc = jnp.zeros((part, 2 * HALF), F32)
        square = jnp.zeros((part, HALF), F32)
        for k in order:
            if k in FETCHED:
                fetch(g, FETCHED.index(k)).wait()
                x = held[g, FETCHED.index(k)]
            else:
                x = chunks[g // 2][k][(g % 2) * slabs : (g % 2 + 1) * slabs, :]
            left, right = from_slabs(x)
            w = serve[pl.ds(sources[k] * spread, spread)].reshape(2 * HALF, 2 * HALF)
            both = jnp.concatenate([left, right], axis=1)
            acc = acc + jnp.dot(both, w, preferred_element_type=F32)
            l32, r32 = left.astype(F32), right.astype(F32)
            square = square + (l32 * l32 + r32 * r32)
        total = jnp.sum(square, axis=1, keepdims=True)
        scale = lax.rsqrt(total * (1.0 / features) + epsilon)
        gate = acc[:, :HALF] * scale
        up = acc[:, HALF:] * scale
        value = gate / (1.0 + jnp.exp(-gate)) * up
        hidden[g * part : (g + 1) * part, :] = value.astype(BF16)


def down_kernel(me, *refs):
    chunks, pieces, out, serve = refs[0:8], refs[8:-2], *refs[-2:]
    sources = offsets_of(me[0])
    join_pieces(me[1], pieces, serve)
    spread = HALF // serve.shape[1]
    part = 8 * CAP
    pairs = ((0, 7), (1, 2), (3, 4), (5, 6))

    def rows_of(source):
        return serve[pl.ds(source * spread, spread)].reshape(HALF, 2 * HALF)

    for g in range(4):
        acc = jnp.zeros((part, 2 * HALF), F32)
        for m, n in pairs:
            h = jnp.concatenate([chunks[k][g * part : (g + 1) * part, :] for k in (m, n)], axis=1)
            w = jnp.concatenate([rows_of(sources[m]), rows_of(sources[n])], axis=0)
            acc = acc + jnp.dot(h, w, preferred_element_type=F32)
        to_slabs(acc, out, 8 * g)


def combine_kernel(rows, gains, returned, mixture):
    n_tok = rows.shape[0]
    slabs, part = 8 * SLAB, 8 * CAP
    sums = [jnp.zeros((n_tok, 2 * HALF), F32) for _ in range(2)]
    for g in range(returned.shape[0] // slabs):
        left, right = from_slabs(returned[g * slabs : (g + 1) * slabs, :])
        both = jnp.concatenate([left, right], axis=1)
        ids = lax.broadcasted_iota(jnp.int32, (n_tok, part), 1) + g * part
        for k in range(2):
            onehot = (ids == rows[:, k : k + 1]).astype(F32).astype(BF16)
            sums[k] = sums[k] + jnp.dot(onehot, both, preferred_element_type=F32)
    mixture[...] = (gains[:, 0:1] * sums[0] + gains[:, 1:2] * sums[1]).astype(BF16)


LIMIT = pltpu.CompilerParams(vmem_limit_bytes=16 * 1024 * 1024)


def in_vmem(*arrays):
    return [pltpu.with_memory_space_constraint(x, pltpu.VMEM) for x in arrays]


def in_hbm(*arrays):
    return [pltpu.with_memory_space_constraint(x, pltpu.HBM) for x in arrays]


def all_to_all(x):
    return lax.all_to_all(x, "fs", split_axis=0, concat_axis=0, tiled=True)


def step(x, shift):
    n = lax.axis_size("tp")
    return lax.ppermute(x, "tp", [(d, (d + shift) % n) for d in range(n)])


def ring(x, end):
    r1, l1 = step(x, 1), step(x, -1)
    r2, l2 = step(r1, 1), step(l1, -1)
    r3, l3 = step(r2, 1), step(l2, -1)
    x4 = step(r3, 1) if end == "r" else step(l3, -1)
    return (x, r1, l1, r2, l2, r3, l3, x4)


def mixture_of_experts(tokens, norm_gain, gate_weight, up_weight, down_weight, routes, route_weights):
    experts, rows_in, cols = gate_weight.shape
    rows_down, down_cols = down_weight.shape[1:]
    n_tok = tokens.shape[0]
    groups = lax.axis_size("grp")
    count = 2 if groups % 2 == 0 else 1
    mine = lax.axis_index("grp") % count
    me = jnp.stack([lax.axis_index("tp"), mine]).astype(jnp.int32)
    smem = pl.BlockSpec(memory_space=pltpu.SMEM)
    vmem = pl.BlockSpec(memory_space=pltpu.VMEM)
    anywhere = pl.BlockSpec(memory_space=pl.ANY)
    slabs = (experts, SLAB, HALF)
    outbound, rows = pl.pallas_call(
        route_kernel,
        in_specs=[anywhere, anywhere],
        out_specs=(vmem, vmem),
        scratch_shapes=[
            pltpu.VMEM((2, n_tok), jnp.int32),
            pltpu.VMEM(tokens.shape, BF16),
            pltpu.SemaphoreType.DMA((2,)),
        ],
        out_shape=(pltpu.VMEM(slabs, BF16), pltpu.VMEM((8, n_tok), jnp.int32)),
        name="route",
        compiler_params=LIMIT,
    )(*in_hbm(routes.T, tokens))
    arrived = all_to_all(outbound).reshape(experts * SLAB, HALF)

    def piece(x, axis):
        size = x.shape[axis] // count
        return lax.dynamic_slice_in_dim(x, mine * size, size, axis)

    def swapped(x):
        if count == 1:
            return [x]
        return [x, lax.ppermute(x, "grp", [(g, g ^ 1) for g in range(groups)])]

    gain = piece(norm_gain, 0)[None, :, None]
    both_low = jnp.concatenate([gain * piece(gate_weight, 1), gain * piece(up_weight, 1)], axis=2)
    weights_low = jnp.concatenate([both_low, piece(down_weight, 1)], axis=1).astype(BF16)
    arrived_weights = all_to_all(weights_low)
    both_pieces = swapped(arrived_weights[:, : rows_in // count])
    down_pieces = swapped(arrived_weights[:, rows_in // count :])
    cut = experts * SLAB // 2
    chunks = ring(arrived[:cut], "r") + ring(arrived[cut:], "l")
    fetched = [n % 8 in FETCHED for n in range(16)]
    hidden = pl.pallas_call(
        ffn_kernel,
        in_specs=[smem] + [anywhere if f else vmem for f in fetched] + [vmem] * count,
        out_specs=vmem,
        out_shape=pltpu.VMEM((experts * CAP, cols), BF16),
        scratch_shapes=[
            pltpu.VMEM((experts, rows_in, 2 * cols), BF16),
            pltpu.VMEM((4, len(FETCHED), 8 * SLAB, HALF), BF16),
            pltpu.SemaphoreType.DMA((4, len(FETCHED))),
        ],
        name="ffn",
        compiler_params=LIMIT,
    )(
        me,
        *[(in_hbm if f else in_vmem)(x)[0] for f, x in zip(fetched, chunks)],
        *in_vmem(*both_pieces),
    )
    expert_out = pl.pallas_call(
        down_kernel,
        in_specs=[smem] + [vmem] * (8 + count),
        out_specs=vmem,
        out_shape=pltpu.VMEM(slabs, BF16),
        scratch_shapes=[pltpu.VMEM((experts, rows_down, down_cols), BF16)],
        name="down",
        compiler_params=LIMIT,
    )(me, *in_vmem(*ring(hidden, "r"), *down_pieces))
    returned = all_to_all(expert_out).reshape(experts * SLAB, HALF)
    mixture = pl.pallas_call(
        combine_kernel,
        in_specs=[vmem] * 3,
        out_specs=vmem,
        out_shape=jax.ShapeDtypeStruct(tokens.shape, BF16),
        name="combine",
        compiler_params=LIMIT,
    )(*in_vmem(rows.T, route_weights, returned))

    def assembled(pieces):
        if count == 1:
            return pieces[0].reshape(1, -1, pieces[0].shape[2])
        own, other = pieces
        both = jnp.where(mine == 0, own, other), jnp.where(mine == 0, other, own)
        return jnp.concatenate(both, axis=1).reshape(1, -1, own.shape[2])

    gate_serve = assembled([x[:, :, :cols] for x in both_pieces])
    up_serve = assembled([x[:, :, cols:] for x in both_pieces])
    return (gate_serve, up_serve, assembled(down_pieces), mixture)


def solution(mesh):
    block = ("grp", "fs")
    return jax.shard_map(
        mixture_of_experts,
        mesh=mesh,
        in_specs=(
            P(block, "tp"),
            P("fs"),
            P(None, "fs", "tp"),
            P(None, "fs", "tp"),
            P(None, "fs", "tp"),
            P(block, None),
            P(block, None),
        ),
        out_specs=(
            P(block, None, "tp"),
            P(block, None, "tp"),
            P(block, None, "tp"),
            P(block, "tp"),
        ),
        check_vma=False,
    )
```

```python
import jax
import jax.numpy as jnp
from jax import lax
from jax.experimental import pallas as pl
from jax.experimental.pallas import tpu as pltpu
from jax.sharding import PartitionSpec as P


CAP = 36
SPREAD = 4
FETCHED = (0, 1, 2)
MAIN = 32
SLAB = 72
HALF = 128
BF16 = jnp.bfloat16
F32 = jnp.float32
epsilon = 1e-06


def tile_row(shape):
    return lax.broadcasted_iota(jnp.int32, shape, len(shape) - 2)


def from_slabs(x):
    x = x.reshape(8, SLAB, HALF)
    left = x[:, :MAIN].reshape(8 * MAIN, HALF)
    right = x[:, MAIN : 2 * MAIN].reshape(8 * MAIN, HALF)
    rest = x[:, 2 * MAIN :].astype(F32).reshape(4, 2, 8, HALF)
    even, odd = rest[:, 0], rest[:, 1]
    low = tile_row((4, 8, HALF)) < CAP - MAIN
    rest_l = jnp.where(low, even, pltpu.roll(odd, 4, 1)).reshape(32, HALF).astype(BF16)
    rest_r = jnp.where(low, pltpu.roll(even, 4, 1), odd).reshape(32, HALF).astype(BF16)
    return jnp.concatenate([left, rest_l], axis=0), jnp.concatenate([right, rest_r], axis=0)


def to_slabs(rows, out, first):
    pairs = 8 * MAIN
    rest_l = rows[pairs:, :HALF].reshape(4, 8, HALF)
    rest_r = rows[pairs:, HALF:].reshape(4, 8, HALF)
    low = tile_row((4, 8, HALF)) < CAP - MAIN
    even = jnp.where(low, rest_l, pltpu.roll(rest_r, 4, 1))
    odd = jnp.where(low, pltpu.roll(rest_l, 4, 1), rest_r)
    rest = jnp.stack([even, odd], axis=1).reshape(8, 8, HALF)
    out[first : first + 8, 0:MAIN, :] = rows[:pairs, :HALF].reshape(8, MAIN, HALF).astype(BF16)
    out[first : first + 8, MAIN : 2 * MAIN, :] = rows[:pairs, HALF:].reshape(8, MAIN, HALF).astype(BF16)
    out[first : first + 8, 2 * MAIN :, :] = rest.astype(BF16)


def route_kernel(routes_in, tokens_in, outbound, rows, routes, tokens, done):
    experts = outbound.shape[0]
    n_tok = tokens.shape[0]
    fetch_routes = pltpu.make_async_copy(routes_in, routes, done.at[0])
    fetch_tokens = pltpu.make_async_copy(tokens_in, tokens, done.at[1])
    fetch_routes.start()
    fetch_tokens.start()
    fetch_routes.wait()
    first, second = routes[0:1, :], routes[1:2, :]
    ids = lax.broadcasted_iota(jnp.int32, (experts, n_tok), 0)
    hit0 = (ids == first).astype(F32)
    hit1 = (ids == second).astype(F32)
    before = (
        lax.broadcasted_iota(jnp.int32, (n_tok, n_tok), 0)
        < lax.broadcasted_iota(jnp.int32, (n_tok, n_tok), 1)
    ).astype(F32).astype(BF16)
    count0 = jnp.dot(hit0.astype(BF16), before, preferred_element_type=F32)
    count1 = jnp.dot(hit1.astype(BF16), before, preferred_element_type=F32)
    count1 = count1 + jnp.sum(hit0, axis=1, keepdims=True)

    def row_of(expert, hit, count):
        slot = jnp.sum(hit * count, axis=0, keepdims=True).astype(jnp.int32)
        base = jnp.right_shift(expert, 3) * (8 * CAP)
        within = jnp.bitwise_and(expert, 7)
        main = within * MAIN + slot
        rest = 8 * MAIN + within * (CAP - MAIN) + (slot - MAIN)
        return base + jnp.where(slot < MAIN, main, rest)

    row0, row1 = row_of(first, hit0, count0), row_of(second, hit1, count1)
    rows[...] = jnp.concatenate([row0, row1] * 4, axis=0)
    part = 8 * CAP
    fetch_tokens.wait()
    for g in range(experts // 8):
        ids = lax.broadcasted_iota(jnp.int32, (part, n_tok), 0) + g * part
        select = jnp.logical_or(ids == row0, ids == row1).astype(F32).astype(BF16)
        out = jnp.dot(select, tokens[...], preferred_element_type=F32)
        to_slabs(out, outbound, 8 * g)


def offsets_of(me):
    n_tp = 8
    return [(me + offset + n_tp) % n_tp for offset in (0, -1, 1, -2, 2, -3, 3, 4)]


def join_pieces(mine, pieces, serve):
    count, rows = len(pieces), pieces[0].shape[1]
    for n, piece in enumerate(pieces):
        place = (mine + n) % count
        serve[:, pl.ds(pl.multiple_of(place * rows, rows), rows), :] = piece[...]


def ffn_kernel(me, *refs):
    chunks, weights, hidden, held, done = (refs[0:8], refs[8:16]), *refs[16:]
    sources = offsets_of(me[0])
    rows = 2 * HALF // SPREAD
    features = weights.shape[0] * rows
    part, slabs = 8 * CAP, 8 * SLAB

    def fetch(g, n):
        source = chunks[g // 2][FETCHED[n]].at[pl.ds((g % 2) * slabs, slabs), :]
        return pltpu.make_async_copy(source, held.at[g, n], done.at[g, n])

    for g in range(4):
        for n in range(len(FETCHED)):
            fetch(g, n).start()
    order = [k for k in range(8) if k not in FETCHED] + list(FETCHED)
    for g in range(4):
        acc = jnp.zeros((part, 2 * HALF), F32)
        square = jnp.zeros((part, HALF), F32)
        for k in order:
            if k in FETCHED:
                fetch(g, FETCHED.index(k)).wait()
                x = held[g, FETCHED.index(k)]
            else:
                x = chunks[g // 2][k][(g % 2) * slabs : (g % 2 + 1) * slabs, :]
            left, right = from_slabs(x)
            w = weights[pl.ds(sources[k] * SPREAD, SPREAD), :rows, :].reshape(2 * HALF, 2 * HALF)
            both = jnp.concatenate([left, right], axis=1)
            acc = acc + jnp.dot(both, w, preferred_element_type=F32)
            l32, r32 = left.astype(F32), right.astype(F32)
            square = square + (l32 * l32 + r32 * r32)
        total = jnp.sum(square, axis=1, keepdims=True)
        scale = lax.rsqrt(total * (1.0 / features) + epsilon)
        gate = acc[:, :HALF] * scale
        up = acc[:, HALF:] * scale
        value = gate / (1.0 + jnp.exp(-gate)) * up
        hidden[g * part : (g + 1) * part, :] = value.astype(BF16)


def down_kernel(me, *refs):
    chunks, pieces, out, serve = refs[0:8], refs[8:-2], *refs[-2:]
    sources = offsets_of(me[0])
    join_pieces(me[1], pieces, serve)
    spread = HALF // serve.shape[1]
    part = 8 * CAP
    pairs = ((0, 7), (1, 2), (3, 4), (5, 6))

    def rows_of(source):
        return serve[pl.ds(source * spread, spread)].reshape(HALF, 2 * HALF)

    for g in range(4):
        acc = jnp.zeros((part, 2 * HALF), F32)
        for m, n in pairs:
            h = jnp.concatenate([chunks[k][g * part : (g + 1) * part, :] for k in (m, n)], axis=1)
            w = jnp.concatenate([rows_of(sources[m]), rows_of(sources[n])], axis=0)
            acc = acc + jnp.dot(h, w, preferred_element_type=F32)
        to_slabs(acc, out, 8 * g)


def combine_kernel(rows, gains_in, returned, mixture, gains, done):
    n_tok = rows.shape[0]
    fetch = pltpu.make_async_copy(gains_in, gains, done)
    fetch.start()
    slabs, part = 8 * SLAB, 8 * CAP
    sums = [jnp.zeros((n_tok, 2 * HALF), F32) for _ in range(2)]
    for g in range(returned.shape[0] // slabs):
        left, right = from_slabs(returned[g * slabs : (g + 1) * slabs, :])
        both = jnp.concatenate([left, right], axis=1)
        ids = lax.broadcasted_iota(jnp.int32, (n_tok, part), 1) + g * part
        for k in range(2):
            onehot = (ids == rows[:, k : k + 1]).astype(F32).astype(BF16)
            sums[k] = sums[k] + jnp.dot(onehot, both, preferred_element_type=F32)
    fetch.wait()
    mixture[...] = (gains[:, 0:1] * sums[0] + gains[:, 1:2] * sums[1]).astype(BF16)


LIMIT = pltpu.CompilerParams(vmem_limit_bytes=16 * 1024 * 1024)


def in_vmem(*arrays):
    return [pltpu.with_memory_space_constraint(x, pltpu.VMEM) for x in arrays]


def in_hbm(*arrays):
    return [pltpu.with_memory_space_constraint(x, pltpu.HBM) for x in arrays]


def all_to_all(x):
    return lax.all_to_all(x, "fs", split_axis=0, concat_axis=0, tiled=True)


def step(x, shift):
    n = lax.axis_size("tp")
    return lax.ppermute(x, "tp", [(d, (d + shift) % n) for d in range(n)])


def ring(x, end):
    r1, l1 = step(x, 1), step(x, -1)
    r2, l2 = step(r1, 1), step(l1, -1)
    r3, l3 = step(r2, 1), step(l2, -1)
    x4 = step(r3, 1) if end == "r" else step(l3, -1)
    return (x, r1, l1, r2, l2, r3, l3, x4)


def mixture_of_experts(tokens, norm_gain, gate_weight, up_weight, down_weight, routes, route_weights):
    experts, rows_in, cols = gate_weight.shape
    rows_down, down_cols = down_weight.shape[1:]
    n_tok = tokens.shape[0]
    groups = lax.axis_size("grp")
    count = 2 if groups % 2 == 0 else 1
    mine = lax.axis_index("grp") % count
    me = jnp.stack([lax.axis_index("tp"), mine]).astype(jnp.int32)
    smem = pl.BlockSpec(memory_space=pltpu.SMEM)
    vmem = pl.BlockSpec(memory_space=pltpu.VMEM)
    anywhere = pl.BlockSpec(memory_space=pl.ANY)
    slabs = (experts, SLAB, HALF)
    outbound, rows = pl.pallas_call(
        route_kernel,
        in_specs=[anywhere, anywhere],
        out_specs=(vmem, vmem),
        scratch_shapes=[
            pltpu.VMEM((2, n_tok), jnp.int32),
            pltpu.VMEM(tokens.shape, BF16),
            pltpu.SemaphoreType.DMA((2,)),
        ],
        out_shape=(pltpu.VMEM(slabs, BF16), pltpu.VMEM((8, n_tok), jnp.int32)),
        name="route",
        compiler_params=LIMIT,
    )(*in_hbm(routes.T, tokens))
    arrived = all_to_all(outbound).reshape(experts * SLAB, HALF)

    def piece(x, axis):
        size = x.shape[axis] // count
        return lax.dynamic_slice_in_dim(x, mine * size, size, axis)

    def swapped(x):
        if count == 1:
            return [x]
        return [x, lax.ppermute(x, "grp", [(g, g ^ 1) for g in range(groups)])]

    gain = norm_gain[None, :, None]
    both_low = jnp.concatenate([gain * gate_weight, gain * up_weight], axis=2)
    weights_low = jnp.concatenate([both_low, piece(down_weight, 1)], axis=1).astype(BF16)
    arrived_weights = all_to_all(weights_low)
    down_pieces = swapped(arrived_weights[:, rows_in:])
    cut = experts * SLAB // 2
    chunks = ring(arrived[:cut], "r") + ring(arrived[cut:], "l")
    fetched = [n % 8 in FETCHED for n in range(16)]
    hidden = pl.pallas_call(
        ffn_kernel,
        in_specs=[smem] + [anywhere if f else vmem for f in fetched] + [vmem],
        out_specs=vmem,
        out_shape=pltpu.VMEM((experts * CAP, cols), BF16),
        scratch_shapes=[
            pltpu.VMEM((4, len(FETCHED), 8 * SLAB, HALF), BF16),
            pltpu.SemaphoreType.DMA((4, len(FETCHED))),
        ],
        name="ffn",
        compiler_params=LIMIT,
    )(
        me,
        *[(in_hbm if f else in_vmem)(x)[0] for f, x in zip(fetched, chunks)],
        *in_vmem(arrived_weights),
    )
    expert_out = pl.pallas_call(
        down_kernel,
        in_specs=[smem] + [vmem] * (8 + count),
        out_specs=vmem,
        out_shape=pltpu.VMEM(slabs, BF16),
        scratch_shapes=[pltpu.VMEM((experts, rows_down, down_cols), BF16)],
        name="down",
        compiler_params=LIMIT,
    )(me, *in_vmem(*ring(hidden, "r"), *down_pieces))
    returned = all_to_all(expert_out).reshape(experts * SLAB, HALF)
    mixture = pl.pallas_call(
        combine_kernel,
        in_specs=[vmem, anywhere, vmem],
        out_specs=vmem,
        scratch_shapes=[pltpu.VMEM(route_weights.shape, F32), pltpu.SemaphoreType.DMA],
        out_shape=jax.ShapeDtypeStruct(tokens.shape, BF16),
        name="combine",
        compiler_params=LIMIT,
    )(*in_vmem(rows.T), *in_hbm(route_weights), *in_vmem(returned))

    def assembled(pieces):
        if count == 1:
            return pieces[0].reshape(1, -1, pieces[0].shape[2])
        own, other = pieces
        both = jnp.where(mine == 0, own, other), jnp.where(mine == 0, other, own)
        return jnp.concatenate(both, axis=1).reshape(1, -1, own.shape[2])

    both_serve = arrived_weights[:, :rows_in].reshape(1, -1, 2 * cols)
    gate_serve, up_serve = both_serve[:, :, :cols], both_serve[:, :, cols:]
    return (gate_serve, up_serve, assembled(down_pieces), mixture)


def solution(mesh):
    block = ("grp", "fs")
    return jax.shard_map(
        mixture_of_experts,
        mesh=mesh,
        in_specs=(
            P(block, "tp"),
            P("fs"),
            P(None, "fs", "tp"),
            P(None, "fs", "tp"),
            P(None, "fs", "tp"),
            P(block, None),
            P(block, None),
        ),
        out_specs=(
            P(block, None, "tp"),
            P(block, None, "tp"),
            P(block, None, "tp"),
            P(block, "tp"),
        ),
        check_vma=False,
    )
```

```python
import jax
import jax.numpy as jnp
from jax import lax
from jax.experimental import pallas as pl
from jax.experimental.pallas import tpu as pltpu
from jax.sharding import PartitionSpec as P


CAP = 36
FETCHED = (0, 1, 2)
MAIN = 32
SLAB = 72
HALF = 128
BF16 = jnp.bfloat16
F32 = jnp.float32
epsilon = 1e-06


def tile_row(shape):
    return lax.broadcasted_iota(jnp.int32, shape, len(shape) - 2)


def from_slabs(x):
    x = x.reshape(8, SLAB, HALF)
    left = x[:, :MAIN].reshape(8 * MAIN, HALF)
    right = x[:, MAIN : 2 * MAIN].reshape(8 * MAIN, HALF)
    rest = x[:, 2 * MAIN :].astype(F32).reshape(4, 2, 8, HALF)
    even, odd = rest[:, 0], rest[:, 1]
    low = tile_row((4, 8, HALF)) < CAP - MAIN
    rest_l = jnp.where(low, even, pltpu.roll(odd, 4, 1)).reshape(32, HALF).astype(BF16)
    rest_r = jnp.where(low, pltpu.roll(even, 4, 1), odd).reshape(32, HALF).astype(BF16)
    return jnp.concatenate([left, rest_l], axis=0), jnp.concatenate([right, rest_r], axis=0)


def to_slabs(rows, out, first):
    pairs = 8 * MAIN
    rest_l = rows[pairs:, :HALF].reshape(4, 8, HALF)
    rest_r = rows[pairs:, HALF:].reshape(4, 8, HALF)
    low = tile_row((4, 8, HALF)) < CAP - MAIN
    even = jnp.where(low, rest_l, pltpu.roll(rest_r, 4, 1))
    odd = jnp.where(low, pltpu.roll(rest_l, 4, 1), rest_r)
    rest = jnp.stack([even, odd], axis=1).reshape(8, 8, HALF)
    out[first : first + 8, 0:MAIN, :] = rows[:pairs, :HALF].reshape(8, MAIN, HALF).astype(BF16)
    out[first : first + 8, MAIN : 2 * MAIN, :] = rows[:pairs, HALF:].reshape(8, MAIN, HALF).astype(BF16)
    out[first : first + 8, 2 * MAIN :, :] = rest.astype(BF16)


def route_kernel(routes_in, tokens_in, outbound, rows, routes, tokens, done):
    experts = outbound.shape[0]
    n_tok = tokens.shape[0]
    fetch_routes = pltpu.make_async_copy(routes_in, routes, done.at[0])
    fetch_tokens = pltpu.make_async_copy(tokens_in, tokens, done.at[1])
    fetch_routes.start()
    fetch_tokens.start()
    fetch_routes.wait()
    first, second = routes[0:1, :], routes[1:2, :]
    ids = lax.broadcasted_iota(jnp.int32, (experts, n_tok), 0)
    hit0 = (ids == first).astype(F32)
    hit1 = (ids == second).astype(F32)
    before = (
        lax.broadcasted_iota(jnp.int32, (n_tok, n_tok), 0)
        < lax.broadcasted_iota(jnp.int32, (n_tok, n_tok), 1)
    ).astype(F32).astype(BF16)
    count0 = jnp.dot(hit0.astype(BF16), before, preferred_element_type=F32)
    count1 = jnp.dot(hit1.astype(BF16), before, preferred_element_type=F32)
    count1 = count1 + jnp.sum(hit0, axis=1, keepdims=True)

    def row_of(expert, hit, count):
        slot = jnp.sum(hit * count, axis=0, keepdims=True).astype(jnp.int32)
        base = jnp.right_shift(expert, 3) * (8 * CAP)
        within = jnp.bitwise_and(expert, 7)
        main = within * MAIN + slot
        rest = 8 * MAIN + within * (CAP - MAIN) + (slot - MAIN)
        return base + jnp.where(slot < MAIN, main, rest)

    row0, row1 = row_of(first, hit0, count0), row_of(second, hit1, count1)
    rows[...] = jnp.concatenate([row0, row1] * 4, axis=0)
    part = 8 * CAP
    fetch_tokens.wait()
    for g in range(experts // 8):
        ids = lax.broadcasted_iota(jnp.int32, (part, n_tok), 0) + g * part
        select = jnp.logical_or(ids == row0, ids == row1).astype(F32).astype(BF16)
        out = jnp.dot(select, tokens[...], preferred_element_type=F32)
        to_slabs(out, outbound, 8 * g)


def offsets_of(me):
    n_tp = 8
    return [(me + offset + n_tp) % n_tp for offset in (0, -1, 1, -2, 2, -3, 3, 4)]


def ffn_kernel(me, *refs):
    chunks, weights, hidden, held, partial, partial_square, done = (refs[0:8], refs[8:16]), *refs[16:]
    sources = offsets_of(me[0])
    features = weights.shape[0]
    part, slabs = 8 * CAP, 8 * SLAB

    def fetch(g, n):
        source = chunks[g // 2][FETCHED[n]].at[pl.ds((g % 2) * slabs, slabs), :]
        return pltpu.make_async_copy(source, held.at[g, n], done.at[g, n])

    def add(acc, square, k, x):
        left, right = from_slabs(x)
        w = weights[pl.ds(pl.multiple_of(sources[k] * 256, 256), 256), :]
        both = jnp.concatenate([left, right], axis=1)
        l32, r32 = left.astype(F32), right.astype(F32)
        dot = jnp.dot(both, w, preferred_element_type=F32)
        return acc + dot, square + (l32 * l32 + r32 * r32)

    for g in range(4):
        for n in range(len(FETCHED)):
            fetch(g, n).start()
    for g in range(4):
        acc = jnp.zeros((part, 2 * HALF), F32)
        square = jnp.zeros((part, HALF), F32)
        for k in range(8):
            if k not in FETCHED:
                x = chunks[g // 2][k][(g % 2) * slabs : (g % 2 + 1) * slabs, :]
                acc, square = add(acc, square, k, x)
        partial[g], partial_square[g] = acc, square
    for g in range(4):
        acc, square = partial[g], partial_square[g]
        for n, k in enumerate(FETCHED):
            fetch(g, n).wait()
            acc, square = add(acc, square, k, held[g, n])
        total = jnp.sum(square, axis=1, keepdims=True)
        scale = lax.rsqrt(total * (1.0 / features) + epsilon)
        gate = acc[:, :HALF] * scale
        up = acc[:, HALF:] * scale
        value = gate / (1.0 + jnp.exp(-gate)) * up
        hidden[g * part : (g + 1) * part, :] = value.astype(BF16)


def down_kernel(me, *refs):
    chunks, weights, out, serve, done = refs[0:8], *refs[8:]
    sources = offsets_of(me[0])
    copy = pltpu.make_async_copy(weights, serve, done)
    copy.start()
    part = 8 * CAP
    pairs = ((0, 7), (1, 2), (3, 4), (5, 6))

    def rows_of(source):
        return weights[pl.ds(pl.multiple_of(source * HALF, HALF), HALF), :]

    for g in range(4):
        acc = jnp.zeros((part, 2 * HALF), F32)
        for m, n in pairs:
            h = jnp.concatenate([chunks[k][g * part : (g + 1) * part, :] for k in (m, n)], axis=1)
            w = jnp.concatenate([rows_of(sources[m]), rows_of(sources[n])], axis=0)
            acc = acc + jnp.dot(h, w, preferred_element_type=F32)
        to_slabs(acc, out, 8 * g)
    copy.wait()


def combine_kernel(rows_in, gains_in, returned, mixture):
    n_tok = rows_in.shape[1]
    rows = rows_in[...].astype(F32).T.astype(jnp.int32)
    gains = jnp.concatenate([gains_in[...]] * 4, axis=0).T
    slabs, part = 8 * SLAB, 8 * CAP
    sums = [jnp.zeros((n_tok, 2 * HALF), F32) for _ in range(2)]
    for g in range(returned.shape[0] // slabs):
        left, right = from_slabs(returned[g * slabs : (g + 1) * slabs, :])
        both = jnp.concatenate([left, right], axis=1)
        ids = lax.broadcasted_iota(jnp.int32, (n_tok, part), 1) + g * part
        for k in range(2):
            onehot = (ids == rows[:, k : k + 1]).astype(F32).astype(BF16)
            sums[k] = sums[k] + jnp.dot(onehot, both, preferred_element_type=F32)
    mixture[...] = (gains[:, 0:1] * sums[0] + gains[:, 1:2] * sums[1]).astype(BF16)


LIMIT = pltpu.CompilerParams(vmem_limit_bytes=16 * 1024 * 1024)


def in_vmem(*arrays):
    return [pltpu.with_memory_space_constraint(x, pltpu.VMEM) for x in arrays]


def in_hbm(*arrays):
    return [pltpu.with_memory_space_constraint(x, pltpu.HBM) for x in arrays]


def all_to_all(x):
    return lax.all_to_all(x, "fs", split_axis=0, concat_axis=0, tiled=True)


def step(x, shift):
    n = lax.axis_size("tp")
    return lax.ppermute(x, "tp", [(d, (d + shift) % n) for d in range(n)])


def ring(x, end):
    r1, l1 = step(x, 1), step(x, -1)
    r2, l2 = step(r1, 1), step(l1, -1)
    r3, l3 = step(r2, 1), step(l2, -1)
    x4 = step(r3, 1) if end == "r" else step(l3, -1)
    return (x, r1, l1, r2, l2, r3, l3, x4)


def mixture_of_experts(tokens, norm_gain, gate_weight, up_weight, down_weight, routes, route_weights):
    experts, _, cols = gate_weight.shape
    n_tok = tokens.shape[0]
    me = lax.axis_index("tp").reshape(1).astype(jnp.int32)
    smem = pl.BlockSpec(memory_space=pltpu.SMEM)
    vmem = pl.BlockSpec(memory_space=pltpu.VMEM)
    anywhere = pl.BlockSpec(memory_space=pl.ANY)
    slabs = (experts, SLAB, HALF)
    outbound, rows = pl.pallas_call(
        route_kernel,
        in_specs=[anywhere, anywhere],
        out_specs=(vmem, vmem),
        scratch_shapes=[
            pltpu.VMEM((2, n_tok), jnp.int32),
            pltpu.VMEM(tokens.shape, BF16),
            pltpu.SemaphoreType.DMA((2,)),
        ],
        out_shape=(pltpu.VMEM(slabs, BF16), pltpu.VMEM((8, n_tok), jnp.int32)),
        name="route",
        compiler_params=LIMIT,
    )(*in_hbm(routes.T, tokens))
    arrived = all_to_all(outbound).reshape(experts * SLAB, HALF)
    gain = norm_gain[None, :, None]
    both_low = jnp.concatenate([gain * gate_weight, gain * up_weight], axis=2).astype(BF16)
    both_low, down_low = lax.optimization_barrier((both_low, down_weight.astype(BF16)))
    both_serve = all_to_all(both_low).reshape(-1, 2 * cols)
    down_rows = all_to_all(down_low).reshape(-1, down_low.shape[2])
    cut = experts * SLAB // 2
    chunks = ring(arrived[:cut], "r") + ring(arrived[cut:], "l")
    fetched = [n % 8 in FETCHED for n in range(16)]
    hidden = pl.pallas_call(
        ffn_kernel,
        in_specs=[smem] + [anywhere if f else vmem for f in fetched] + [vmem],
        out_specs=vmem,
        out_shape=pltpu.VMEM((experts * CAP, cols), BF16),
        scratch_shapes=[
            pltpu.VMEM((4, len(FETCHED), 8 * SLAB, HALF), BF16),
            pltpu.VMEM((4, 8 * CAP, 2 * HALF), F32),
            pltpu.VMEM((4, 8 * CAP, HALF), F32),
            pltpu.SemaphoreType.DMA((4, len(FETCHED))),
        ],
        name="ffn",
        compiler_params=LIMIT,
    )(
        me,
        *[(in_hbm if f else in_vmem)(x)[0] for f, x in zip(fetched, chunks)],
        *in_vmem(both_serve),
    )
    expert_out, down_serve = pl.pallas_call(
        down_kernel,
        in_specs=[smem] + [vmem] * 9,
        out_specs=(vmem, anywhere),
        out_shape=(pltpu.VMEM(slabs, BF16), jax.ShapeDtypeStruct(down_rows.shape, BF16)),
        scratch_shapes=[pltpu.SemaphoreType.DMA],
        name="down",
        compiler_params=LIMIT,
    )(me, *in_vmem(*ring(hidden, "r"), down_rows))
    returned = all_to_all(expert_out).reshape(experts * SLAB, HALF)
    mixture = pl.pallas_call(
        combine_kernel,
        in_specs=[vmem] * 3,
        out_specs=vmem,
        out_shape=jax.ShapeDtypeStruct(tokens.shape, BF16),
        name="combine",
        compiler_params=LIMIT,
    )(*in_vmem(rows, route_weights.T, returned))
    gate_serve, up_serve = both_serve[None, :, :cols], both_serve[None, :, cols:]
    return (gate_serve, up_serve, down_serve[None], mixture)


def solution(mesh):
    block = ("grp", "fs")
    return jax.shard_map(
        mixture_of_experts,
        mesh=mesh,
        in_specs=(
            P(block, "tp"),
            P("fs"),
            P(None, "fs", "tp"),
            P(None, "fs", "tp"),
            P(None, "fs", "tp"),
            P(block, None),
            P(block, None),
        ),
        out_specs=(
            P(block, None, "tp"),
            P(block, None, "tp"),
            P(block, None, "tp"),
            P(block, "tp"),
        ),
        check_vma=False,
    )
```

```python
import jax
import jax.numpy as jnp
from jax import lax
from jax.experimental import pallas as pl
from jax.experimental.pallas import tpu as pltpu
from jax.sharding import PartitionSpec as P


CAP = 36
SPREAD = 4
WAITING = (0, 1, 2, 3, 4, 5, 6)
MAIN = 32
SLAB = 72
HALF = 128
BF16 = jnp.bfloat16
F32 = jnp.float32
epsilon = 1e-06


def tile_row(shape):
    return lax.broadcasted_iota(jnp.int32, shape, len(shape) - 2)


def from_slabs(x):
    x = x.reshape(8, SLAB, HALF)
    left = x[:, :MAIN].reshape(8 * MAIN, HALF)
    right = x[:, MAIN : 2 * MAIN].reshape(8 * MAIN, HALF)
    rest = x[:, 2 * MAIN :].astype(F32).reshape(4, 2, 8, HALF)
    even, odd = rest[:, 0], rest[:, 1]
    low = tile_row((4, 8, HALF)) < CAP - MAIN
    rest_l = jnp.where(low, even, pltpu.roll(odd, 4, 1)).reshape(32, HALF).astype(BF16)
    rest_r = jnp.where(low, pltpu.roll(even, 4, 1), odd).reshape(32, HALF).astype(BF16)
    return jnp.concatenate([left, rest_l], axis=0), jnp.concatenate([right, rest_r], axis=0)


def to_slabs(rows, out, first):
    pairs = 8 * MAIN
    rest_l = rows[pairs:, :HALF].reshape(4, 8, HALF)
    rest_r = rows[pairs:, HALF:].reshape(4, 8, HALF)
    low = tile_row((4, 8, HALF)) < CAP - MAIN
    even = jnp.where(low, rest_l, pltpu.roll(rest_r, 4, 1))
    odd = jnp.where(low, pltpu.roll(rest_l, 4, 1), rest_r)
    rest = jnp.stack([even, odd], axis=1).reshape(8, 8, HALF)
    out[first : first + 8, 0:MAIN, :] = rows[:pairs, :HALF].reshape(8, MAIN, HALF).astype(BF16)
    out[first : first + 8, MAIN : 2 * MAIN, :] = rows[:pairs, HALF:].reshape(8, MAIN, HALF).astype(BF16)
    out[first : first + 8, 2 * MAIN :, :] = rest.astype(BF16)


def route_kernel(routes_in, tokens_in, outbound, rows, routes, tokens, done):
    experts = outbound.shape[0]
    n_tok = tokens.shape[0]
    fetch_routes = pltpu.make_async_copy(routes_in, routes, done.at[0])
    fetch_tokens = pltpu.make_async_copy(tokens_in, tokens, done.at[1])
    fetch_routes.start()
    fetch_tokens.start()
    fetch_routes.wait()
    first, second = routes[0:1, :], routes[1:2, :]
    ids = lax.broadcasted_iota(jnp.int32, (experts, n_tok), 0)
    hit0 = (ids == first).astype(F32)
    hit1 = (ids == second).astype(F32)
    before = (
        lax.broadcasted_iota(jnp.int32, (n_tok, n_tok), 0)
        < lax.broadcasted_iota(jnp.int32, (n_tok, n_tok), 1)
    ).astype(F32).astype(BF16)
    count0 = jnp.dot(hit0.astype(BF16), before, preferred_element_type=F32)
    count1 = jnp.dot(hit1.astype(BF16), before, preferred_element_type=F32)
    count1 = count1 + jnp.sum(hit0, axis=1, keepdims=True)

    def row_of(expert, hit, count):
        slot = jnp.sum(hit * count, axis=0, keepdims=True).astype(jnp.int32)
        base = jnp.right_shift(expert, 3) * (8 * CAP)
        within = jnp.bitwise_and(expert, 7)
        main = within * MAIN + slot
        rest = 8 * MAIN + within * (CAP - MAIN) + (slot - MAIN)
        return base + jnp.where(slot < MAIN, main, rest)

    row0, row1 = row_of(first, hit0, count0), row_of(second, hit1, count1)
    rows[...] = jnp.concatenate([row0, row1] * 4, axis=0)
    part = 8 * CAP
    fetch_tokens.wait()
    for g in range(experts // 8):
        ids = lax.broadcasted_iota(jnp.int32, (part, n_tok), 0) + g * part
        select = jnp.logical_or(ids == row0, ids == row1).astype(F32).astype(BF16)
        out = jnp.dot(select, tokens[...], preferred_element_type=F32)
        to_slabs(out, outbound, 8 * g)


def offsets_of(me):
    n_tp = 8
    return [(me + offset + n_tp) % n_tp for offset in (0, -1, 1, -2, 2, -3, 3, 4)]


def join_pieces(mine, pieces, serve):
    rows = pieces[0].shape[1]
    if len(pieces) == 1:
        serve[...] = pieces[0][...]
        return
    own, other = pieces[0][...], pieces[1][...]
    serve[:, :rows, :] = jnp.where(mine == 0, own, other)
    serve[:, rows:, :] = jnp.where(mine == 0, other, own)


def ffn_kernel(me, *refs):
    chunks, weights, hidden = (refs[0:8], refs[8:16]), *refs[16:]
    sources = offsets_of(me[0])
    rows = 2 * HALF // SPREAD
    features = weights.shape[0] * rows
    part, slabs = 8 * CAP, 8 * SLAB
    for g in range(4):
        acc = jnp.zeros((part, 2 * HALF), F32)
        square = jnp.zeros((part, HALF), F32)
        for source, chunk in zip(sources, chunks[g // 2]):
            left, right = from_slabs(chunk[(g % 2) * slabs : (g % 2 + 1) * slabs, :])
            w = weights[pl.ds(source * SPREAD, SPREAD), :rows, :].reshape(2 * HALF, 2 * HALF)
            both = jnp.concatenate([left, right], axis=1)
            acc = acc + jnp.dot(both, w, preferred_element_type=F32)
            l32, r32 = left.astype(F32), right.astype(F32)
            square = square + (l32 * l32 + r32 * r32)
        total = jnp.sum(square, axis=1, keepdims=True)
        scale = lax.rsqrt(total * (1.0 / features) + epsilon)
        gate = acc[:, :HALF] * scale
        up = acc[:, HALF:] * scale
        value = gate / (1.0 + jnp.exp(-gate)) * up
        hidden[g * part : (g + 1) * part, :] = value.astype(BF16)


def down_kernel(me, *refs):
    chunks, pieces, out, serve_out, serve, done = refs[0:8], refs[8:-4], *refs[-4:]
    sources = offsets_of(me[0])
    join_pieces(me[1], pieces, serve)
    copy = pltpu.make_async_copy(serve, serve_out, done)
    copy.start()
    spread = HALF // serve.shape[1]
    part = 8 * CAP
    pairs = ((0, 7), (1, 2), (3, 4), (5, 6))

    def rows_of(source):
        return serve[pl.ds(source * spread, spread)].reshape(HALF, 2 * HALF)

    for g in range(4):
        acc = jnp.zeros((part, 2 * HALF), F32)
        for m, n in pairs:
            h = jnp.concatenate([chunks[k][g * part : (g + 1) * part, :] for k in (m, n)], axis=1)
            w = jnp.concatenate([rows_of(sources[m]), rows_of(sources[n])], axis=0)
            acc = acc + jnp.dot(h, w, preferred_element_type=F32)
        to_slabs(acc, out, 8 * g)
    copy.wait()


def combine_kernel(rows_in, gains_in, returned, mixture):
    n_tok = rows_in.shape[1]
    rows = rows_in[...].astype(F32).T.astype(jnp.int32)
    gains = jnp.concatenate([gains_in[...]] * 4, axis=0).T
    slabs, part = 8 * SLAB, 8 * CAP
    sums = [jnp.zeros((n_tok, 2 * HALF), F32) for _ in range(2)]
    for g in range(returned.shape[0] // slabs):
        left, right = from_slabs(returned[g * slabs : (g + 1) * slabs, :])
        both = jnp.concatenate([left, right], axis=1)
        ids = lax.broadcasted_iota(jnp.int32, (n_tok, part), 1) + g * part
        for k in range(2):
            onehot = (ids == rows[:, k : k + 1]).astype(F32).astype(BF16)
            sums[k] = sums[k] + jnp.dot(onehot, both, preferred_element_type=F32)
    mixture[...] = (gains[:, 0:1] * sums[0] + gains[:, 1:2] * sums[1]).astype(BF16)


LIMIT = pltpu.CompilerParams(vmem_limit_bytes=16 * 1024 * 1024)


def in_vmem(*arrays):
    return [pltpu.with_memory_space_constraint(x, pltpu.VMEM) for x in arrays]


def in_hbm(*arrays):
    return [pltpu.with_memory_space_constraint(x, pltpu.HBM) for x in arrays]


def all_to_all(x):
    return lax.all_to_all(x, "fs", split_axis=0, concat_axis=0, tiled=True)


def step(x, shift):
    n = lax.axis_size("tp")
    return lax.ppermute(x, "tp", [(d, (d + shift) % n) for d in range(n)])


def crossed_step(r3, l3):
    n, devices = lax.axis_size("tp"), lax.axis_size("fs")
    x = jnp.where(lax.axis_index("fs") % 2 == 0, r3, l3)
    pairs = [(f * n + d, f * n + (d + 1 - 2 * (f % 2)) % n) for f in range(devices) for d in range(n)]
    return lax.ppermute(x, ("fs", "tp"), pairs)


def ring(x, end):
    r1, l1 = step(x, 1), step(x, -1)
    r2, l2 = step(r1, 1), step(l1, -1)
    r3, l3 = step(r2, 1), step(l2, -1)
    if end == "both":
        x4 = crossed_step(r3, l3)
    else:
        x4 = step(r3, 1) if end == "r" else step(l3, -1)
    return (x, r1, l1, r2, l2, r3, l3, x4)


def mixture_of_experts(tokens, norm_gain, gate_weight, up_weight, down_weight, routes, route_weights):
    experts, rows_in, cols = gate_weight.shape
    rows_down, down_cols = down_weight.shape[1:]
    n_tok = tokens.shape[0]
    groups = lax.axis_size("grp")
    count = 2 if groups % 2 == 0 else 1
    mine = lax.axis_index("grp") % count
    me = jnp.stack([lax.axis_index("tp"), mine]).astype(jnp.int32)
    smem = pl.BlockSpec(memory_space=pltpu.SMEM)
    vmem = pl.BlockSpec(memory_space=pltpu.VMEM)
    anywhere = pl.BlockSpec(memory_space=pl.ANY)
    slabs = (experts, SLAB, HALF)
    outbound, rows = pl.pallas_call(
        route_kernel,
        in_specs=[anywhere, anywhere],
        out_specs=(vmem, vmem),
        scratch_shapes=[
            pltpu.VMEM((2, n_tok), jnp.int32),
            pltpu.VMEM(tokens.shape, BF16),
            pltpu.SemaphoreType.DMA((2,)),
        ],
        out_shape=(pltpu.VMEM(slabs, BF16), pltpu.VMEM((8, n_tok), jnp.int32)),
        name="route",
        compiler_params=LIMIT,
    )(*in_hbm(routes.T, tokens))
    arrived = all_to_all(outbound).reshape(experts * SLAB, HALF)

    def piece(x, axis):
        size = x.shape[axis] // count
        return lax.dynamic_slice_in_dim(x, mine * size, size, axis)

    def swapped(x):
        if count == 1:
            return [x]
        return [x, lax.ppermute(x, "grp", [(g, g ^ 1) for g in range(groups)])]

    gain = norm_gain[None, :, None]
    both_low = jnp.concatenate([gain * gate_weight, gain * up_weight], axis=2)
    weights_low = jnp.concatenate([both_low, piece(down_weight, 1)], axis=1).astype(BF16)
    arrived_weights = all_to_all(weights_low)
    down_pieces = swapped(arrived_weights[:, rows_in:])
    cut = experts * SLAB // 2
    chunks = ring(arrived[:cut], "r") + ring(arrived[cut:], "l")
    fetched = [n % 8 in WAITING for n in range(16)]
    hidden = pl.pallas_call(
        ffn_kernel,
        in_specs=[smem] + [vmem] * 17,
        out_specs=vmem,
        out_shape=pltpu.VMEM((experts * CAP, cols), BF16),
        name="ffn",
        compiler_params=LIMIT,
    )(
        me,
        *[(in_hbm if f else in_vmem)(x)[0] for f, x in zip(fetched, chunks)],
        *in_vmem(arrived_weights),
    )
    down_shape = (experts, rows_down, down_cols)
    expert_out, down_serve = pl.pallas_call(
        down_kernel,
        in_specs=[smem] + [vmem] * (8 + count),
        out_specs=(vmem, anywhere),
        out_shape=(pltpu.VMEM(slabs, BF16), jax.ShapeDtypeStruct(down_shape, BF16)),
        scratch_shapes=[pltpu.VMEM(down_shape, BF16), pltpu.SemaphoreType.DMA],
        name="down",
        compiler_params=LIMIT,
    )(me, *in_vmem(*ring(hidden, "both"), *down_pieces))
    returned = all_to_all(expert_out).reshape(experts * SLAB, HALF)
    mixture = pl.pallas_call(
        combine_kernel,
        in_specs=[vmem] * 3,
        out_specs=vmem,
        out_shape=jax.ShapeDtypeStruct(tokens.shape, BF16),
        name="combine",
        compiler_params=LIMIT,
    )(*in_vmem(rows, route_weights.T, returned))

    both_serve = arrived_weights[:, :rows_in].reshape(1, -1, 2 * cols)
    gate_serve, up_serve = both_serve[:, :, :cols], both_serve[:, :, cols:]
    return (gate_serve, up_serve, down_serve.reshape(1, -1, down_cols), mixture)


def solution(mesh):
    block = ("grp", "fs")
    return jax.shard_map(
        mixture_of_experts,
        mesh=mesh,
        in_specs=(
            P(block, "tp"),
            P("fs"),
            P(None, "fs", "tp"),
            P(None, "fs", "tp"),
            P(None, "fs", "tp"),
            P(block, None),
            P(block, None),
        ),
        out_specs=(
            P(block, None, "tp"),
            P(block, None, "tp"),
            P(block, None, "tp"),
            P(block, "tp"),
        ),
        check_vma=False,
    )
```

```python
import jax
import jax.numpy as jnp
from jax import lax
from jax.experimental import pallas as pl
from jax.experimental.pallas import tpu as pltpu
from jax.sharding import PartitionSpec as P


CAP = 36
SPREAD = 4
WAITING = (0, 1, 2)
MAIN = 32
SLAB = 72
HALF = 128
BF16 = jnp.bfloat16
F32 = jnp.float32
epsilon = 1e-06


def tile_row(shape):
    return lax.broadcasted_iota(jnp.int32, shape, len(shape) - 2)


def from_slabs(x):
    x = x.reshape(8, SLAB, HALF)
    left = x[:, :MAIN].reshape(8 * MAIN, HALF)
    right = x[:, MAIN : 2 * MAIN].reshape(8 * MAIN, HALF)
    rest = x[:, 2 * MAIN :].astype(F32).reshape(4, 2, 8, HALF)
    even, odd = rest[:, 0], rest[:, 1]
    low = tile_row((4, 8, HALF)) < CAP - MAIN
    rest_l = jnp.where(low, even, pltpu.roll(odd, 4, 1)).reshape(32, HALF).astype(BF16)
    rest_r = jnp.where(low, pltpu.roll(even, 4, 1), odd).reshape(32, HALF).astype(BF16)
    return jnp.concatenate([left, rest_l], axis=0), jnp.concatenate([right, rest_r], axis=0)


def to_slabs(rows, out, first):
    pairs = 8 * MAIN
    rest_l = rows[pairs:, :HALF].reshape(4, 8, HALF)
    rest_r = rows[pairs:, HALF:].reshape(4, 8, HALF)
    low = tile_row((4, 8, HALF)) < CAP - MAIN
    even = jnp.where(low, rest_l, pltpu.roll(rest_r, 4, 1))
    odd = jnp.where(low, pltpu.roll(rest_l, 4, 1), rest_r)
    rest = jnp.stack([even, odd], axis=1).reshape(8, 8, HALF)
    out[first : first + 8, 0:MAIN, :] = rows[:pairs, :HALF].reshape(8, MAIN, HALF).astype(BF16)
    out[first : first + 8, MAIN : 2 * MAIN, :] = rows[:pairs, HALF:].reshape(8, MAIN, HALF).astype(BF16)
    out[first : first + 8, 2 * MAIN :, :] = rest.astype(BF16)


def route_kernel(routes_in, tokens_in, outbound, rows, routes, tokens, done):
    experts = outbound.shape[0]
    n_tok = tokens.shape[0]
    fetch_routes = pltpu.make_async_copy(routes_in, routes, done.at[0])
    fetch_tokens = pltpu.make_async_copy(tokens_in, tokens, done.at[1])
    fetch_routes.start()
    fetch_tokens.start()
    fetch_routes.wait()
    first, second = routes[0:1, :], routes[1:2, :]
    ids = lax.broadcasted_iota(jnp.int32, (experts, n_tok), 0)
    hit0 = (ids == first).astype(F32)
    hit1 = (ids == second).astype(F32)
    before = (
        lax.broadcasted_iota(jnp.int32, (n_tok, n_tok), 0)
        < lax.broadcasted_iota(jnp.int32, (n_tok, n_tok), 1)
    ).astype(F32).astype(BF16)
    count0 = jnp.dot(hit0.astype(BF16), before, preferred_element_type=F32)
    count1 = jnp.dot(hit1.astype(BF16), before, preferred_element_type=F32)
    count1 = count1 + jnp.sum(hit0, axis=1, keepdims=True)

    def row_of(expert, hit, count):
        slot = jnp.sum(hit * count, axis=0, keepdims=True).astype(jnp.int32)
        base = jnp.right_shift(expert, 3) * (8 * CAP)
        within = jnp.bitwise_and(expert, 7)
        main = within * MAIN + slot
        rest = 8 * MAIN + within * (CAP - MAIN) + (slot - MAIN)
        return base + jnp.where(slot < MAIN, main, rest)

    row0, row1 = row_of(first, hit0, count0), row_of(second, hit1, count1)
    rows[...] = jnp.concatenate([row0, row1] * 4, axis=0)
    part = 8 * CAP
    fetch_tokens.wait()
    for g in range(experts // 8):
        ids = lax.broadcasted_iota(jnp.int32, (part, n_tok), 0) + g * part
        select = jnp.logical_or(ids == row0, ids == row1).astype(F32).astype(BF16)
        out = jnp.dot(select, tokens[...], preferred_element_type=F32)
        to_slabs(out, outbound, 8 * g)


def offsets_of(me):
    n_tp = 8
    return [(me + offset + n_tp) % n_tp for offset in (0, -1, 1, -2, 2, -3, 3, 4)]


def join_pieces(mine, pieces, serve):
    rows = pieces[0].shape[1]
    if len(pieces) == 1:
        serve[...] = pieces[0][...]
        return
    own, other = pieces[0][...], pieces[1][...]
    serve[:, :rows, :] = jnp.where(mine == 0, own, other)
    serve[:, rows:, :] = jnp.where(mine == 0, other, own)


def ffn_kernel(me, *refs):
    chunks, weights, hidden = (refs[0:8], refs[8:16]), *refs[16:]
    sources = offsets_of(me[0])
    rows = 2 * HALF // SPREAD
    features = weights.shape[0] * rows
    part, slabs = 8 * CAP, 8 * SLAB
    for g in range(4):
        acc = jnp.zeros((part, 2 * HALF), F32)
        square = jnp.zeros((part, HALF), F32)
        for source, chunk in zip(sources, chunks[g // 2]):
            left, right = from_slabs(chunk[(g % 2) * slabs : (g % 2 + 1) * slabs, :])
            w = weights[pl.ds(source * SPREAD, SPREAD), :rows, :].reshape(2 * HALF, 2 * HALF)
            both = jnp.concatenate([left, right], axis=1)
            acc = acc + jnp.dot(both, w, preferred_element_type=F32)
            l32, r32 = left.astype(F32), right.astype(F32)
            square = square + (l32 * l32 + r32 * r32)
        total = jnp.sum(square, axis=1, keepdims=True)
        scale = lax.rsqrt(total * (1.0 / features) + epsilon)
        gate = acc[:, :HALF] * scale
        up = acc[:, HALF:] * scale
        value = gate / (1.0 + jnp.exp(-gate)) * up
        hidden[g * part : (g + 1) * part, :] = value.astype(BF16)


def down_kernel(me, *refs):
    chunks, pieces, out, serve_out, serve, done = refs[0:8], refs[8:-4], *refs[-4:]
    sources = offsets_of(me[0])
    join_pieces(me[1], pieces, serve)
    copy = pltpu.make_async_copy(serve, serve_out, done)
    copy.start()
    spread = HALF // serve.shape[1]
    part = 8 * CAP
    pairs = ((0, 7), (1, 2), (3, 4), (5, 6))

    def rows_of(source):
        return serve[pl.ds(source * spread, spread)].reshape(HALF, 2 * HALF)

    for g in range(4):
        acc = jnp.zeros((part, 2 * HALF), F32)
        for m, n in pairs:
            h = jnp.concatenate([chunks[k][g * part : (g + 1) * part, :] for k in (m, n)], axis=1)
            w = jnp.concatenate([rows_of(sources[m]), rows_of(sources[n])], axis=0)
            acc = acc + jnp.dot(h, w, preferred_element_type=F32)
        to_slabs(acc, out, 8 * g)
    copy.wait()


def combine_kernel(rows_in, gains_in, returned, mixture):
    n_tok = rows_in.shape[1]
    rows = rows_in[...].astype(F32).T.astype(jnp.int32)
    gains = jnp.concatenate([gains_in[...]] * 4, axis=0).T
    slabs, part = 8 * SLAB, 8 * CAP
    sums = [jnp.zeros((n_tok, 2 * HALF), F32) for _ in range(2)]
    for g in range(returned.shape[0] // slabs):
        left, right = from_slabs(returned[g * slabs : (g + 1) * slabs, :])
        both = jnp.concatenate([left, right], axis=1)
        ids = lax.broadcasted_iota(jnp.int32, (n_tok, part), 1) + g * part
        for k in range(2):
            onehot = (ids == rows[:, k : k + 1]).astype(F32).astype(BF16)
            sums[k] = sums[k] + jnp.dot(onehot, both, preferred_element_type=F32)
    mixture[...] = (gains[:, 0:1] * sums[0] + gains[:, 1:2] * sums[1]).astype(BF16)


LIMIT = pltpu.CompilerParams(vmem_limit_bytes=16 * 1024 * 1024)


def in_vmem(*arrays):
    return [pltpu.with_memory_space_constraint(x, pltpu.VMEM) for x in arrays]


def in_hbm(*arrays):
    return [pltpu.with_memory_space_constraint(x, pltpu.HBM) for x in arrays]


def all_to_all(x):
    return lax.all_to_all(x, "fs", split_axis=0, concat_axis=0, tiled=True)


def step(x, shift):
    n = lax.axis_size("tp")
    return lax.ppermute(x, "tp", [(d, (d + shift) % n) for d in range(n)])


def ring(x, end):
    r1, l1 = step(x, 1), step(x, -1)
    r2, l2 = step(r1, 1), step(l1, -1)
    r3, l3 = step(r2, 1), step(l2, -1)
    x4 = step(r3, 1) if end == "r" else step(l3, -1)
    return (x, r1, l1, r2, l2, r3, l3, x4)


def mixture_of_experts(tokens, norm_gain, gate_weight, up_weight, down_weight, routes, route_weights):
    experts, rows_in, cols = gate_weight.shape
    rows_down, down_cols = down_weight.shape[1:]
    n_tok = tokens.shape[0]
    groups = lax.axis_size("grp")
    count = 2 if groups % 2 == 0 else 1
    mine = lax.axis_index("grp") % count
    me = jnp.stack([lax.axis_index("tp"), mine]).astype(jnp.int32)
    smem = pl.BlockSpec(memory_space=pltpu.SMEM)
    vmem = pl.BlockSpec(memory_space=pltpu.VMEM)
    anywhere = pl.BlockSpec(memory_space=pl.ANY)
    slabs = (experts, SLAB, HALF)
    outbound, rows = pl.pallas_call(
        route_kernel,
        in_specs=[anywhere, anywhere],
        out_specs=(vmem, vmem),
        scratch_shapes=[
            pltpu.VMEM((2, n_tok), jnp.int32),
            pltpu.VMEM(tokens.shape, BF16),
            pltpu.SemaphoreType.DMA((2,)),
        ],
        out_shape=(pltpu.VMEM(slabs, BF16), pltpu.VMEM((8, n_tok), jnp.int32)),
        name="route",
        compiler_params=LIMIT,
    )(*in_hbm(routes.T, tokens))
    arrived = all_to_all(outbound).reshape(experts * SLAB, HALF)

    def piece(x, axis):
        size = x.shape[axis] // count
        return lax.dynamic_slice_in_dim(x, mine * size, size, axis)

    def swapped(x):
        if count == 1:
            return [x]
        return [x, lax.ppermute(x, "grp", [(g, g ^ 1) for g in range(groups)])]

    gain = norm_gain[None, :, None]
    both_low = jnp.concatenate([gain * gate_weight, gain * up_weight], axis=2)
    weights_low = jnp.concatenate([both_low, piece(down_weight, 1)], axis=1).astype(BF16)
    arrived_weights = all_to_all(weights_low)
    down_pieces = swapped(arrived_weights[:, rows_in:])
    cut = experts * SLAB // 2
    chunks = ring(arrived[:cut], "r") + ring(arrived[cut:], "l")
    fetched = [n % 8 in WAITING for n in range(16)]
    hidden = pl.pallas_call(
        ffn_kernel,
        in_specs=[smem] + [vmem] * 17,
        out_specs=vmem,
        out_shape=pltpu.VMEM((experts * CAP, cols), BF16),
        name="ffn",
        compiler_params=LIMIT,
    )(
        me,
        *[(in_hbm if f else in_vmem)(x)[0] for f, x in zip(fetched, chunks)],
        *in_vmem(arrived_weights),
    )
    down_shape = (experts, rows_down, down_cols)
    expert_out, down_serve = pl.pallas_call(
        down_kernel,
        in_specs=[smem] + [vmem] * (8 + count),
        out_specs=(vmem, anywhere),
        out_shape=(pltpu.VMEM(slabs, BF16), jax.ShapeDtypeStruct(down_shape, BF16)),
        scratch_shapes=[pltpu.VMEM(down_shape, BF16), pltpu.SemaphoreType.DMA],
        name="down",
        compiler_params=LIMIT,
    )(me, *in_vmem(*ring(hidden, "r"), *down_pieces))
    returned = all_to_all(expert_out).reshape(experts * SLAB, HALF)
    mixture = pl.pallas_call(
        combine_kernel,
        in_specs=[vmem] * 3,
        out_specs=vmem,
        out_shape=jax.ShapeDtypeStruct(tokens.shape, BF16),
        name="combine",
        compiler_params=LIMIT,
    )(*in_vmem(rows, route_weights.T, returned))

    both_serve = arrived_weights[:, :rows_in].reshape(1, -1, 2 * cols)
    gate_serve, up_serve = both_serve[:, :, :cols], both_serve[:, :, cols:]
    return (gate_serve, up_serve, down_serve.reshape(1, -1, down_cols), mixture)


def solution(mesh):
    block = ("grp", "fs")
    return jax.shard_map(
        mixture_of_experts,
        mesh=mesh,
        in_specs=(
            P(block, "tp"),
            P("fs"),
            P(None, "fs", "tp"),
            P(None, "fs", "tp"),
            P(None, "fs", "tp"),
            P(block, None),
            P(block, None),
        ),
        out_specs=(
            P(block, None, "tp"),
            P(block, None, "tp"),
            P(block, None, "tp"),
            P(block, "tp"),
        ),
        check_vma=False,
    )
```
